512 devices in a mesh: kv: 16 (over y, x), tp: 32 (over z, core).
Axes of the slice: x: 4, y: 4, z: 16, core: 2. Of those that a mesh axis runs over, the one named last changes fastest.
Arguments:
- resid: bfloat16 [128, 4096], P('tp', 'kv'), may hold values from -35 to 35
- attn_gain: bfloat16 [4096], replicated, may hold values from 0.099609375 to 1.8984375
- w_query_nope: bfloat16 [4096, 8192], P('kv', 'tp'), may hold values from -0.09375 to 0.09375
- w_query_rope: bfloat16 [4096, 4096], P('kv', 'tp'), may hold values from -0.09375 to 0.09375
- w_latent: bfloat16 [4096, 512], P('kv'), may hold values from -0.09375 to 0.09375
- w_key_rope: bfloat16 [4096, 64], replicated, may hold values from -0.09375 to 0.09375
- latent_gain: bfloat16 [512], replicated, may hold values from 0.099609375 to 1.8984375
- key_up: bfloat16 [512, 64, 128], P(None, 'tp'), may hold values from -0.5 to 0.5
- value_up: bfloat16 [512, 64, 128], P(None, 'tp'), may hold values from -0.25 to 0.25
- w_out: bfloat16 [8192, 4096], P('tp', 'kv'), may hold values from -4 to 4
- post_gain: bfloat16 [4096], replicated, may hold values from 0.099609375 to 1.8984375
- mlp_gain: bfloat16 [4096], replicated, may hold values from 0.099609375 to 1.8984375
- w_gate: bfloat16 [4096, 11008], P('kv', 'tp'), may hold values from -3 to 3
- w_up: bfloat16 [4096, 11008], P('kv', 'tp'), may hold values from -3 to 3
- w_down: bfloat16 [11008, 4096], P('tp', 'kv'), may hold values from -0.0546875 to 0.0546875
- cache_latent: bfloat16 [128, 8192, 512], P('tp', 'kv'), may hold values from -6 to 6
- cache_rope_key: bfloat16 [128, 8192, 64], P('tp', 'kv'), may hold values from -740 to 740
Outputs:
- next_resid: bfloat16 [128, 4096], P('tp', 'kv')
- new_latent: bfloat16 [128, 512], P('tp')
- new_rope_key: bfloat16 [128, 64], P('tp')
The draws below stay inside these ranges and needn't reach their ends.
All inputs are finite; a program needn't handle non-finite values.
Results may differ from the reference program's by a relative error of at most 0.035.
Values may be sent and summed in bfloat16 or wider, within the bound.
A program may use at most 64 MiB of HBM per device.

```python
import jax
import jax.numpy as jnp
from jax import lax

D = 4096
H = 64
NOPE = 128
ROPE = 64
VD = 128
LAT = 512
FF = 11008
POS_DEV = 512
BATCH = 128
CTX = 8192
N_KV = 16


def rising_profile(length, factor):
    place = (jnp.arange(length, dtype=jnp.float32) + 0.5) / length
    profile = jnp.exp(jnp.log(factor) * (place - 0.5))
    return profile / jnp.sqrt(jnp.mean(profile * profile))


def draw_resid(key, part):
    key_base, key_rows = jax.random.split(jax.random.fold_in(key, 101))
    column_pos = jnp.arange(D, dtype=jnp.float32) / D
    column_scale = 0.5 * jnp.exp(jnp.log(4.0) * column_pos)[None, :]
    base_draw = jnp.clip(jax.random.normal(key_base, (BATCH, D), jnp.float32), -6.0, 6.0)
    row_scale = jnp.exp(jax.random.uniform(key_rows, (BATCH, 1), jnp.float32, -0.5, 0.5))
    return (base_draw * column_scale * row_scale).astype(jnp.bfloat16)


def draw_w_out(key, part):
    factor = 6.0
    base_draw = jnp.clip(jax.random.normal(jax.random.fold_in(key, 103), (H * VD, D), jnp.float32), -6.0, 6.0)
    scaled = base_draw * rising_profile(H * VD, factor)[:, None] * rising_profile(D, factor)[None, :]
    return (scaled * (H * VD) ** (-0.5)).astype(jnp.bfloat16)


def rising_rows(key, factor):
    base_draw = jnp.clip(jax.random.normal(key, (D, FF), jnp.float32), -6.0, 6.0)
    return (base_draw * rising_profile(D, factor)[:, None] * D ** (-0.5)).astype(jnp.bfloat16)


def draw_w_gate(key, part):
    factor = 6.0
    return rising_rows(jax.random.fold_in(key, 107), factor)


def draw_w_up(key, part):
    factor = 6.0
    return rising_rows(jax.random.fold_in(key, 109), factor)


def draw_cache_rope_key(key, part):
    key_base = jax.random.fold_in(jax.random.fold_in(key, 113), 0)
    base_draw = jnp.clip(jax.random.normal(key_base, (BATCH, CTX, ROPE), jnp.float32), -6.0, 6.0)
    return base_draw.astype(jnp.bfloat16)


def block_levels(stream_key, shape, cuts, smallest, top_value):
    def one(dim, blocks):
        draws = jax.random.uniform(jax.random.fold_in(jax.random.fold_in(stream_key, 6), dim), (blocks,), jnp.float32, smallest / len(cuts), top_value / len(cuts))
        return jnp.repeat(jnp.exp(draws), shape[dim] // blocks).reshape((-1,) + (1,) * (len(shape) - dim - 1))

    loudness = one(*cuts[0])
    for cut in cuts[1:]:
        loudness = loudness * one(*cut)
    return loudness


def noise(key, shape, width, reach, pieces=(), kind=jnp.bfloat16):
    values = jax.random.normal(key, shape, jnp.float32) * width
    if len(pieces) > 0:
        values = block_levels(key, shape, pieces, -0.22, 0.18) * values
    return jnp.clip(values, min=-reach, max=reach).astype(kind)


def setup_inputs(seed: int = 0) -> dict:
    streams_of = jax.random.split(jax.random.key(seed), 18)
    resid = draw_resid(jax.random.fold_in(streams_of[17], 71), 0)
    attn_gain = jnp.clip(1.0 + 0.18 * jax.random.normal(streams_of[1], (D,), jnp.float32), 0.099609375, 1.8984375).astype(jnp.bfloat16)
    w_query_nope = noise(streams_of[2], (D, H * NOPE), D ** -0.5, 0.09375, ((0, 16), (1, 32)))
    w_query_rope = noise(streams_of[3], (D, H * ROPE), D ** -0.5, 0.09375, ((0, 16), (1, 32)))
    w_latent = noise(streams_of[4], (D, LAT), D ** -0.5, 0.09375, ((0, 16),))
    w_key_rope = noise(streams_of[5], (D, ROPE), D ** -0.5, 0.09375)
    latent_gain = jnp.clip(1.0 + 0.18 * jax.random.normal(streams_of[6], (LAT,), jnp.float32), 0.099609375, 1.8984375).astype(jnp.bfloat16)
    key_up = noise(streams_of[7], (LAT, H, NOPE), NOPE ** -0.5, 0.5, ((1, 32),))
    value_up = noise(streams_of[8], (LAT, H, VD), LAT ** -0.5, 0.25, ((1, 32),))
    w_out = draw_w_out(jax.random.fold_in(streams_of[17], 71), 0)
    post_gain = jnp.clip(1.0 + 0.18 * jax.random.normal(streams_of[10], (D,), jnp.float32), 0.099609375, 1.8984375).astype(jnp.bfloat16)
    mlp_gain = jnp.clip(1.0 + 0.18 * jax.random.normal(streams_of[11], (D,), jnp.float32), 0.099609375, 1.8984375).astype(jnp.bfloat16)
    w_gate = draw_w_gate(jax.random.fold_in(streams_of[17], 71), 0)
    w_up = draw_w_up(jax.random.fold_in(streams_of[17], 71), 0)
    w_down = noise(streams_of[14], (FF, D), FF ** -0.5, 0.0546875, ((0, 32), (1, 16)))
    cache_latent = noise(streams_of[15], (BATCH, CTX, LAT), 1.0, 6.0, ((0, 32), (1, 16)))
    cache_rope_key = draw_cache_rope_key(jax.random.fold_in(streams_of[17], 71), 0)
    return dict(resid=resid, attn_gain=attn_gain, w_query_nope=w_query_nope, w_query_rope=w_query_rope, w_latent=w_latent, w_key_rope=w_key_rope, latent_gain=latent_gain, key_up=key_up, value_up=value_up, w_out=w_out, post_gain=post_gain, mlp_gain=mlp_gain, w_gate=w_gate, w_up=w_up, w_down=w_down, cache_latent=cache_latent, cache_rope_key=cache_rope_key)


EPS = 1e-06
THETA = 10000.0

def rotate(vector, position):
    half_width = vector.shape[-1] // 2
    frequency = THETA ** (-jnp.arange(half_width, dtype=jnp.float32) / half_width)
    angles = jnp.asarray(position, jnp.float32) * frequency
    cos_table, sin_table = (jnp.cos(angles), jnp.sin(angles))
    lower_half, upper_half = (vector[..., :half_width], vector[..., half_width:])
    return jnp.concatenate([lower_half * cos_table - upper_half * sin_table, lower_half * sin_table + upper_half * cos_table], axis=-1)

def reference(resid, attn_gain, w_query_nope, w_query_rope, w_latent, w_key_rope, latent_gain, key_up, value_up, w_out, post_gain, mlp_gain, w_gate, w_up, w_down, cache_latent, cache_rope_key):
    batch_rows = resid.shape[0]
    head_count = key_up.shape[1]
    context = cache_latent.shape[1]
    latent_width = cache_latent.shape[2]
    score_scale = (key_up.shape[2] + cache_rope_key.shape[2]) ** (-0.5)
    resid_float = resid.astype(jnp.float32)
    normed_a = (resid_float * attn_gain.astype(jnp.float32)).astype(jnp.bfloat16)
    scale_in = lax.rsqrt(lax.optimization_barrier(jnp.mean(resid_float * resid_float, axis=1, keepdims=True)) + EPS)
    q_nope = (jnp.dot(normed_a, w_query_nope, preferred_element_type=jnp.float32) * scale_in).astype(jnp.bfloat16)
    q_rope_raw = jnp.dot(normed_a, w_query_rope, preferred_element_type=jnp.float32) * scale_in
    q_rope = rotate(q_rope_raw.reshape(batch_rows, head_count, -1), context).astype(jnp.bfloat16)
    latent_raw = jnp.dot(normed_a, w_latent, preferred_element_type=jnp.float32)
    new_latent = (latent_raw * lax.rsqrt(lax.optimization_barrier(jnp.mean(latent_raw * latent_raw, axis=1, keepdims=True)) + EPS) * latent_gain.astype(jnp.float32)).astype(jnp.bfloat16)
    key_raw = jnp.dot(normed_a, w_key_rope, preferred_element_type=jnp.float32) * scale_in
    new_rope_key = rotate(key_raw, context).astype(jnp.bfloat16)
    q_lat = jnp.einsum('bhd,chd->bhc', q_nope.reshape(batch_rows, head_count, -1).astype(jnp.float32), key_up.astype(jnp.float32)).astype(jnp.bfloat16)

    def attend(item):
        query_lat, query_rope, keys, rope_keys, own_latent, own_rope = item
        scores = (jnp.dot(query_lat, keys.T, preferred_element_type=jnp.float32) + jnp.dot(query_rope, rope_keys.T, preferred_element_type=jnp.float32)) * score_scale
        own_score = (jnp.dot(query_lat, own_latent, preferred_element_type=jnp.float32) + jnp.dot(query_rope, own_rope, preferred_element_type=jnp.float32)) * score_scale
        peak = jnp.maximum(lax.optimization_barrier(jnp.max(scores, axis=1)), own_score)
        probs = jnp.exp(scores - peak[:, None])
        own_prob = jnp.exp(own_score - peak)
        totals = lax.optimization_barrier(jnp.sum(probs, axis=1)) + own_prob
        weights = probs.astype(jnp.bfloat16).reshape(head_count, N_KV, POS_DEV)
        blocks = keys.reshape(N_KV, POS_DEV, latent_width)
        partial_value = jnp.einsum('hjp,jpc->hjc', weights.astype(jnp.float32), blocks.astype(jnp.float32))
        partial_value = partial_value.astype(jnp.bfloat16).astype(jnp.float32)
        summed = lax.optimization_barrier(jnp.sum(partial_value, axis=1)) + own_prob[:, None] * own_latent.astype(jnp.float32)[None, :]
        return (summed / totals[:, None]).astype(jnp.bfloat16)
    o_lat = lax.map(attend, (q_lat, q_rope, cache_latent, cache_rope_key, new_latent, new_rope_key))
    o_heads = jnp.einsum('bhc,che->bhe', o_lat.astype(jnp.float32), value_up.astype(jnp.float32))
    o_heads = o_heads.astype(jnp.bfloat16).reshape(batch_rows, -1)
    attended = jnp.dot(o_heads, w_out, preferred_element_type=jnp.float32)
    post_part = attended * lax.rsqrt(lax.optimization_barrier(jnp.mean(attended * attended, axis=1, keepdims=True)) + EPS) * post_gain.astype(jnp.float32)
    resid_mid = (resid_float + post_part).astype(jnp.bfloat16)
    mid_float = resid_mid.astype(jnp.float32)
    normed_m = (mid_float * mlp_gain.astype(jnp.float32)).astype(jnp.bfloat16)
    scale_mid = lax.rsqrt(lax.optimization_barrier(jnp.mean(mid_float * mid_float, axis=1, keepdims=True)) + EPS)
    gate = jnp.dot(normed_m, w_gate, preferred_element_type=jnp.float32) * scale_mid
    up_part = jnp.dot(normed_m, w_up, preferred_element_type=jnp.float32) * scale_mid
    hidden = (jax.nn.silu(gate) * up_part).astype(jnp.bfloat16)
    next_resid = (mid_float + jnp.dot(hidden, w_down, preferred_element_type=jnp.float32)).astype(jnp.bfloat16)
    return (next_resid, new_latent, new_rope_key)
```

```python
import functools

import jax
import jax.numpy as jnp
import numpy as np
from jax import lax
from jax.experimental import pallas as pl
from jax.experimental.pallas import tpu as pltpu
from jax.sharding import PartitionSpec as P

EPS = 1e-06
THETA = 10000.0
MESH = pl.DeviceIdType.MESH
F32 = jnp.float32
BF16 = jnp.bfloat16
NN = (((1,), (0,)), ((), ()))
NT = (((1,), (1,)), ((), ()))


def dot(a, b, dims=NN):
    return lax.dot_general(a, b, dims, preferred_element_type=F32)


def halves(value):
    high = value.astype(BF16).astype(F32)
    return high, (value - high).astype(BF16).astype(F32)


def put(ref, rows, value, first=0):
    for c in range(value.shape[1] // 128):
        ref[first + c, rows, :] = value[:, 128 * c : 128 * (c + 1)]


def get(ref, rows):
    return jnp.concatenate([ref[c, rows, :] for c in range(ref.shape[0])], axis=1)


def lanes(shape):
    return lax.broadcasted_iota(jnp.int32, shape, len(shape) - 1)


def rotate(vector, table):
    lower = lanes(vector.shape) % 64 < 32
    partner = jnp.where(lower, pltpu.roll(vector, 96, 1), pltpu.roll(vector, 32, 1))
    return vector * table[0:1, :] + partner * table[1:2, :]


def rotation_table(position):
    frequency = THETA ** (-np.arange(32, dtype=np.float64) / 32)
    angles = position * frequency
    cos, sin = np.cos(angles), np.sin(angles)
    return np.stack(
        [np.tile(np.concatenate([cos, cos]), 2), np.tile(np.concatenate([-sin, sin]), 2)]
    ).astype(np.float32)


INPUTS = (
    "resid",
    "attn_gain",
    "post_gain",
    "mlp_gain",
    "latent_gain",
    "table",
    "wqn",
    "wqr",
    "wl",
    "wkr",
    "ku",
    "vu",
    "wo",
    "wg",
    "wu",
    "wd",
    "cl",
    "cr",
)


def kernel(n_kv, n_tp, *refs):
    n_in = len(INPUTS)
    hbm = dict(zip(INPUTS, refs[:n_in]))
    out_resid, out_latent, out_key = refs[n_in : n_in + 3]
    scratch = refs[n_in + 3 :]
    v = dict(zip(INPUTS, scratch[:n_in]))
    (
        load_sem,
        f1, sb_l, rb_l, rb1, f2, sb2, rb2, f3, sb3, rb3, fq, rb_q, sb4, rb4, f5, sb5, rb5, fo, rb6,
        f7, sb7, rb7, sb8, rb8, mid, rb9, f10, sb10, rb10, sb11, rb11, rb12, sb12, g1, nl,
        tp_send, tp_recv, kv_send, kv_recv, q_recv, o_recv,
    ) = scratch[n_in:]

    k, t = lax.axis_index("kv"), lax.axis_index("tp")
    own = v["resid"].shape[0]
    batch = own * n_tp
    width = v["resid"].shape[1]
    model = width * n_kv
    lat = v["cl"].shape[2]
    quarters = n_kv // own
    share = batch // n_kv
    heads = 2 * n_tp
    heads_q = heads // quarters
    tp_q = n_tp // quarters
    ff = v["wg"].shape[0]
    scale = (v["ku"].shape[2] + 64) ** (-0.5)
    slot, group = lax.rem(k, own), lax.div(k, own)

    loads = {}
    for at, name in enumerate(INPUTS):
        source = hbm[name]
        if name == "wkr":
            source = source.at[:, pl.ds(pl.multiple_of(k * width, width), width)]
        loads[name] = pltpu.make_async_copy(source, v[name], load_sem.at[at])
        loads[name].start()

    barrier = pltpu.get_barrier_semaphore()

    @pl.loop(1, n_tp)
    def _(i):
        pl.semaphore_signal(barrier, inc=1, device_id={"kv": k, "tp": lax.rem(t + i, n_tp)}, device_id_type=MESH)

    @pl.loop(1, n_kv)
    def _(i):
        pl.semaphore_signal(barrier, inc=1, device_id={"kv": lax.rem(k + i, n_kv), "tp": t}, device_id_type=MESH)

    def send(src, dst, send_sem, recv_sem, kv, tp):
        pltpu.make_async_remote_copy(
            src_ref=src,
            dst_ref=dst,
            send_sem=send_sem,
            recv_sem=recv_sem,
            device_id={"kv": kv, "tp": tp},
            device_id_type=MESH,
        ).start()

    def over_tp(src_of, dst, phase):
        @pl.loop(1, n_tp)
        def _(i):
            to = lax.rem(t + i, n_tp)
            send(src_of(to), dst, tp_send.at[phase], tp_recv.at[phase], k, to)

    def over_kv(src_of, dst, phase, recv=None):
        @pl.loop(1, n_kv)
        def _(i):
            to = lax.rem(k + i, n_kv)
            send(src_of(to), dst, kv_send.at[phase], kv_recv.at[phase] if recv is None else recv, to, t)

    def take(ref, sem):
        pltpu.make_async_copy(ref, ref, sem).wait()

    def take_tp(ref, phase):
        take(ref.at[pl.ds(0, n_tp - 1)], tp_recv.at[phase])

    def take_kv(ref, phase):
        take(ref.at[pl.ds(0, n_kv - 1)], kv_recv.at[phase])

    for name in ("attn_gain", "post_gain", "mlp_gain", "resid", "wl", "wkr", "latent_gain", "table"):
        loads[name].wait()

    def block_of(name):
        g1[...] = v[name][...].astype(F32)
        per = width // 128
        return jnp.concatenate([g1[pl.ds(k * per + j, 1), :] for j in range(per)], axis=1)

    attn_gain, post_gain, mlp_gain = block_of("attn_gain"), block_of("post_gain"), block_of("mlp_gain")
    resid = v["resid"][...].astype(F32)
    own_normed = (resid * attn_gain).astype(BF16)
    sb_l[:, 0:lat] = dot(own_normed, v["wl"][...])
    key_part = dot(own_normed, v["wkr"][...], NT)
    square = jnp.sum(resid * resid, axis=1, keepdims=True)
    sb_l[:, lat : lat + 128] = jnp.concatenate([key_part, jnp.broadcast_to(square, (own, 64))], axis=1)

    pl.semaphore_wait(barrier, n_tp + n_kv - 2)

    over_tp(lambda to: v["resid"], rb1.at[t], 0)
    over_kv(lambda to: sb_l, rb_l.at[k], 0)
    rb1[t] = v["resid"][...]
    rb_l[k] = sb_l[...]
    for name in INPUTS:
        if name in ("wqn", "wqr", "ku", "vu", "wo", "wg", "wu", "wd"):
            loads[name].wait()
    take_tp(rb1, 0)
    for j in range(n_tp):
        f1[own * j : own * (j + 1), :] = rb1[j].astype(F32)
    rows = f1[...]
    normed = (rows * attn_gain).astype(BF16)
    high, low = halves(jnp.sum(rows * rows, axis=1, keepdims=True))
    qw = v["wqn"].shape[1]
    every = slice(None)
    put(f2, every, dot(normed, v["wqn"][...]))
    put(f2, every, dot(normed, v["wqr"][...]), qw // 128)
    put(f2, every, jnp.where(lanes((batch, 128)) < 64, high, low), qw // 128 + 1)
    for j in range(n_kv):
        sb2[j] = get(f2, pl.ds(j, share, stride=n_kv)).astype(BF16)
    over_kv(lambda to: sb2.at[to], rb2.at[k], 1)
    rb2[k] = sb2[k]

    take_kv(rb_l, 0)
    total = rb_l[0]
    for j in range(1, n_kv):
        total = total + rb_l[j]
    latent = total[:, 0:lat]
    gain_rows = v["latent_gain"][...].astype(F32)
    latent_gain = jnp.concatenate([gain_rows[j : j + 1, :] for j in range(lat // 128)], axis=1)
    new_latent = (
        latent * lax.rsqrt(jnp.mean(latent * latent, axis=1, keepdims=True) + EPS) * latent_gain
    ).astype(BF16)
    out_latent[...] = new_latent
    key = total[:, lat : lat + 128]
    own_scale = lax.rsqrt(key[:, 64:65] / model + EPS)
    table = v["table"][...]
    new_key = rotate(key * own_scale, table).astype(BF16)
    out_key[...] = new_key[:, 0:64]
    nl[:, 0:lat] = new_latent.astype(F32)
    nl[:, lat : lat + 128] = jnp.where(lanes((own, 128)) < 64, new_key.astype(F32), 0.0)

    take_kv(rb2, 1)
    total = rb2[0].astype(F32)
    for j in range(1, n_kv):
        total = total + rb2[j].astype(F32)
    squares = total[:, qw + 128 : qw + 129] + total[:, qw + 192 : qw + 193]
    scale_in = lax.rsqrt(squares / model + EPS)
    q_nope = (total[:, 0:qw] * scale_in).astype(BF16)
    q_rope = rotate(total[:, qw : qw + 128] * scale_in, table)
    for h in range(2):
        spot = pl.ds(h, share, stride=2)
        put(f3, spot, dot(q_nope[:, 128 * h : 128 * (h + 1)], v["ku"][h], NT))
        turned = q_rope if h == 0 else pltpu.roll(q_rope, 64, 1)
        put(f3, spot, jnp.where(lanes((share, 128)) < 64, turned, 0.0), lat // 128)
    for i in range(share):
        sb3[i] = get(f3, slice(2 * i, 2 * i + 2)).astype(BF16)
    @pl.loop(0, share)
    def _(i):
        to = quarters * i + group

        @pl.when(to != t)
        def _():
            send(sb3.at[i], rb3.at[t], tp_send.at[1], tp_recv.at[1], k, to)

        @pl.when(to == t)
        def _():
            rb3[t] = sb3[i]

    gathers_q = lax.rem(t, quarters) == group

    @pl.when(gathers_q)
    def _():
        take_tp(rb3, 1)
        for j in range(n_tp):
            fq[2 * j : 2 * j + 2, :] = rb3[j].astype(F32)
        rb_q[slot] = fq[...].astype(BF16)
        over_kv(lambda to: rb_q.at[slot], rb_q.at[slot], 2, q_recv.at[slot])

    loads["cl"].wait()
    loads["cr"].wait()
    for s in range(own):
        @pl.when(k != own * lax.rem(t, quarters) + s)
        def _():
            take(rb_q.at[s], q_recv.at[s])

        keys = v["cl"][s]
        scores = (dot(rb_q[s, :, 0:lat], keys, NT) + dot(rb_q[s, :, lat : lat + 64], v["cr"][s])) * scale
        peak_high, peak_low = halves(jnp.max(scores, axis=1, keepdims=True))
        probs = jnp.exp(scores - (peak_high + peak_low))
        sum_high, sum_low = halves(jnp.sum(probs, axis=1, keepdims=True))
        sb4[s, :, 0:lat] = dot(probs.astype(BF16), keys).astype(BF16)
        lane = lanes((heads, 128))
        sb4[s, :, lat : lat + 128] = jnp.where(
            lane < 32, peak_high, jnp.where(lane < 64, peak_low, jnp.where(lane < 96, sum_high, sum_low))
        ).astype(BF16)
        for q in range(quarters):
            to = own * q + s

            @pl.when(k != to)
            def _():
                send(sb4.at[s, pl.ds(heads_q * q, heads_q)], rb4.at[k], kv_send.at[3], kv_recv.at[3], to, t)

            @pl.when(k == to)
            def _():
                rb4[k] = sb4[s, heads_q * q : heads_q * (q + 1), :]

    query = rb_q[slot, pl.ds(pl.multiple_of(group * heads_q, heads_q), heads_q), :].astype(F32)
    mine = nl[pl.ds(slot, 1), :]
    own_score = jnp.sum(query * mine, axis=1, keepdims=True) * scale
    take_kv(rb4, 3)
    peaks, sums = [], []
    top = own_score
    for j in range(n_kv):
        stats = rb4[j, :, lat : lat + 128].astype(F32)
        peaks.append(stats[:, 0:1] + stats[:, 32:33])
        sums.append(stats[:, 64:65] + stats[:, 96:97])
        top = jnp.maximum(top, peaks[-1])
    own_prob = jnp.exp(own_score - top)
    totals = own_prob
    summed = own_prob * mine[:, 0:lat]
    for j in range(n_kv):
        weight = jnp.exp(peaks[j] - top)
        totals = totals + sums[j] * weight
        summed = summed + rb4[j, :, 0:lat].astype(F32) * weight
    f5[...] = summed / totals
    for i in range(tp_q):
        sb5[i] = f5[2 * i : 2 * i + 2, :].astype(BF16)

    @pl.loop(0, tp_q)
    def _(i):
        to = tp_q * group + i

        @pl.when(to != t)
        def _():
            send(sb5.at[i], rb5.at[t], tp_send.at[2], tp_recv.at[2], k, to)

        @pl.when(to == t)
        def _():
            rb5[t] = sb5[i]

    gathers_o = lax.div(t, tp_q) == group

    @pl.when(gathers_o)
    def _():
        take_tp(rb5, 2)
        for j in range(n_tp):
            put(fo, slice(2 * j, 2 * j + 2), rb5[j].astype(F32))
        terms = [dot(get(fo, pl.ds(h, n_tp, stride=2)).astype(BF16), v["vu"][h]).astype(BF16) for h in range(2)]
        rb6[slot] = jnp.concatenate(terms, axis=1)
        over_kv(lambda to: rb6.at[slot], rb6.at[slot], 4, o_recv.at[slot])

    for s in range(own):
        @pl.when(k != own * lax.div(t, tp_q) + s)
        def _():
            take(rb6.at[s], o_recv.at[s])

        put(f7, slice(n_tp * s, n_tp * (s + 1)), dot(rb6[s], v["wo"][...]))
    for j in range(n_tp):
        sb7[j] = get(f7, pl.ds(j, own, stride=n_tp)).astype(BF16)
    over_tp(lambda to: sb7.at[to], rb7.at[t], 3)
    rb7[t] = sb7[t]
    take_tp(rb7, 3)
    attended = jnp.sum(rb7[...].astype(F32), axis=0)
    sb8[...] = jnp.broadcast_to(jnp.sum(attended * attended, axis=1, keepdims=True), sb8.shape)
    over_kv(lambda to: sb8, rb8.at[k], 5)
    rb8[k] = sb8[...]
    take_kv(rb8, 5)
    post_square = jnp.sum(rb8[...], axis=0)[:, 0:1]
    mid[...] = (resid + attended * lax.rsqrt(post_square / model + EPS) * post_gain).astype(BF16)
    over_tp(lambda to: mid, rb9.at[t], 4)
    rb9[t] = mid[...]
    take_tp(rb9, 4)
    for j in range(n_tp):
        f1[own * j : own * (j + 1), :] = rb9[j].astype(F32)
    rows = f1[...]
    normed = (rows * mlp_gain).astype(BF16)
    high, low = halves(jnp.sum(rows * rows, axis=1, keepdims=True))
    padded = -(-ff // 128) * 128
    free = padded - ff
    f10[:, padded - 128 : padded] = jnp.where(lanes((batch, 128)) < 128 - free // 2, high, low)
    f10[:, 2 * padded - 128 : 2 * padded] = jnp.zeros((batch, 128), F32)
    f10[:, 0:ff] = dot(normed, v["wg"][...], NT)
    f10[:, padded : padded + ff] = dot(normed, v["wu"][...], NT)
    for j in range(n_kv):
        sb10[j] = f10[share * j : share * (j + 1), :].astype(BF16)
    over_kv(lambda to: sb10.at[to], rb10.at[k], 6)
    rb10[k] = sb10[k]
    take_kv(rb10, 6)
    total = rb10[0].astype(F32)
    for j in range(1, n_kv):
        total = total + rb10[j].astype(F32)
    squares = total[:, ff : ff + 1] + total[:, padded - 1 : padded]
    scale_mid = lax.rsqrt(squares / model + EPS)
    gate, up = total[:, 0:padded] * scale_mid, total[:, padded : 2 * padded] * scale_mid
    hidden = gate / (1.0 + jnp.exp(-gate)) * up
    sb11[...] = jnp.where(lanes((share, padded)) < ff, hidden, 0.0).astype(BF16)
    over_kv(lambda to: sb11, rb11.at[k], 7)
    rb11[k] = sb11[...]
    take_kv(rb11, 7)
    everything = rb11[...].astype(F32).reshape(batch, padded).astype(BF16)
    f1[...] = dot(everything[:, 0:ff], v["wd"][...])
    for j in range(n_tp):
        sb12[j] = f1[own * j : own * (j + 1), :].astype(BF16)
    over_tp(lambda to: sb12.at[to], rb12.at[t], 5)
    rb12[t] = sb12[t]
    take_tp(rb12, 5)
    out_resid[...] = (mid[...].astype(F32) + jnp.sum(rb12[...].astype(F32), axis=0)).astype(BF16)

    for phase, ref in ((0, rb1), (3, rb7), (4, rb9), (5, rb12)):
        take(ref.at[pl.ds(0, n_tp - 1)], tp_send.at[phase])
    for phase, ref in ((0, rb_l), (1, rb2), (3, rb4), (5, rb8), (6, rb10), (7, rb11)):
        take(ref.at[pl.ds(0, n_kv - 1)], kv_send.at[phase])
    for phase, ref, count, inside in ((1, rb3, share, gathers_q), (2, rb5, tp_q, gathers_o)):
        @pl.when(inside)
        def _():
            take(ref.at[pl.ds(0, count - 1)], tp_send.at[phase])

        @pl.when(jnp.logical_not(inside))
        def _():
            take(ref.at[pl.ds(0, count)], tp_send.at[phase])

    for phase, ref, inside in ((2, rb_q, gathers_q), (4, rb6, gathers_o)):
        @pl.when(inside)
        def _():
            @pl.loop(1, n_kv)
            def _(i):
                take(ref.at[0], kv_send.at[phase])


def body(
    resid, attn_gain, w_query_nope, w_query_rope, w_latent, w_key_rope, latent_gain, key_up, value_up,
    w_out, post_gain, mlp_gain, w_gate, w_up, w_down, cache_latent, cache_rope_key,
):
    n_kv, n_tp = lax.axis_size("kv"), lax.axis_size("tp")
    own, width = resid.shape
    batch, share = own * n_tp, own * n_tp // n_kv
    lat, positions = cache_latent.shape[2], cache_latent.shape[1]
    quarters = n_kv // own
    heads = 2 * n_tp
    heads_q, tp_q = heads // quarters, n_tp // quarters
    ff = w_gate.shape[1]
    padded = -(-ff // 128) * 128
    qw = w_query_nope.shape[1]
    operands = (
        resid,
        attn_gain.reshape(-1, 128),
        post_gain.reshape(-1, 128),
        mlp_gain.reshape(-1, 128),
        latent_gain.reshape(-1, 128),
        jnp.asarray(rotation_table(positions * n_kv)),
        w_query_nope,
        w_query_rope,
        w_latent,
        w_key_rope.T,
        key_up.transpose(1, 0, 2),
        value_up.transpose(1, 0, 2),
        w_out,
        w_gate.T,
        w_up.T,
        w_down,
        cache_latent,
        cache_rope_key.swapaxes(1, 2),
    )
    local = [pltpu.VMEM(o.shape, o.dtype) for o in operands]
    local[9] = pltpu.VMEM((64, width), BF16)
    wide = lat + 128
    dma = pltpu.SemaphoreType.DMA
    scratch = local + [
        dma((len(INPUTS),)),
        pltpu.VMEM((batch, width), F32),
        pltpu.VMEM((own, wide), F32),
        pltpu.VMEM((n_kv, own, wide), F32),
        pltpu.VMEM((n_tp, own, width), BF16),
        pltpu.VMEM((qw // 128 + 2, batch, 128), F32),
        pltpu.VMEM((n_kv, share, qw + 256), BF16),
        pltpu.VMEM((n_kv, share, qw + 256), BF16),
        pltpu.VMEM((wide // 128, 2 * share, 128), F32),
        pltpu.VMEM((share, 2, wide), BF16),
        pltpu.VMEM((n_tp, 2, wide), BF16),
        pltpu.VMEM((heads, wide), F32),
        pltpu.VMEM((own, heads, wide), BF16),
        pltpu.VMEM((own, heads, wide), BF16),
        pltpu.VMEM((n_kv, heads_q, wide), BF16),
        pltpu.VMEM((heads_q, lat), F32),
        pltpu.VMEM((tp_q, 2, lat), BF16),
        pltpu.VMEM((n_tp, 2, lat), BF16),
        pltpu.VMEM((lat // 128, heads, 128), F32),
        pltpu.VMEM((own, n_tp, 256), BF16),
        pltpu.VMEM((width // 128, batch, 128), F32),
        pltpu.VMEM((n_tp, own, width), BF16),
        pltpu.VMEM((n_tp, own, width), BF16),
        pltpu.VMEM((own, 128), F32),
        pltpu.VMEM((n_kv, own, 128), F32),
        pltpu.VMEM((own, width), BF16),
        pltpu.VMEM((n_tp, own, width), BF16),
        pltpu.VMEM((batch, 2 * padded), F32),
        pltpu.VMEM((n_kv, share, 2 * padded), BF16),
        pltpu.VMEM((n_kv, share, 2 * padded), BF16),
        pltpu.VMEM((share, padded), BF16),
        pltpu.VMEM((n_kv, share, padded), BF16),
        pltpu.VMEM((n_tp, own, width), BF16),
        pltpu.VMEM((n_tp, own, width), BF16),
        pltpu.VMEM((attn_gain.shape[0] // 128, 128), F32),
        pltpu.VMEM((own, wide), F32),
        dma((6,)),
        dma((6,)),
        dma((8,)),
        dma((8,)),
        dma((own,)),
        dma((own,)),
    ]
    return pl.pallas_call(
        functools.partial(kernel, n_kv, n_tp),
        out_shape=(
            jax.ShapeDtypeStruct((own, width), BF16),
            jax.ShapeDtypeStruct((own, lat), BF16),
            jax.ShapeDtypeStruct((own, 64), BF16),
        ),
        in_specs=[pl.BlockSpec(memory_space=pl.ANY)] * len(operands),
        out_specs=(pl.BlockSpec(memory_space=pltpu.VMEM),) * 3,
        scratch_shapes=scratch,
        compiler_params=pltpu.CompilerParams(
            collective_id=0, has_side_effects=True, vmem_limit_bytes=67043328
        ),
    )(*operands)


def solution(mesh):
    placed = (
        P("tp", "kv"),
        P(),
        P("kv", "tp"),
        P("kv", "tp"),
        P("kv", None),
        P(),
        P(),
        P(None, "tp", None),
        P(None, "tp", None),
        P("tp", "kv"),
        P(),
        P(),
        P("kv", "tp"),
        P("kv", "tp"),
        P("tp", "kv"),
        P("tp", "kv", None),
        P("tp", "kv", None),
    )
    return jax.shard_map(
        body,
        mesh=mesh,
        in_specs=placed,
        out_specs=(P("tp", "kv"), P("tp", None), P("tp", None)),
        check_vma=False,
    )
```

```python
import functools

import jax
import jax.numpy as jnp
import numpy as np
from jax import lax
from jax.experimental import pallas as pl
from jax.experimental.pallas import tpu as pltpu
from jax.sharding import PartitionSpec as P

EPS = 1e-06
THETA = 10000.0
MESH = pl.DeviceIdType.MESH
F32 = jnp.float32
BF16 = jnp.bfloat16
NN = (((1,), (0,)), ((), ()))
NT = (((1,), (1,)), ((), ()))


def dot(a, b, dims=NN):
    return lax.dot_general(a, b, dims, preferred_element_type=F32)


def halves(value):
    high = value.astype(BF16).astype(F32)
    return high, (value - high).astype(BF16).astype(F32)


def put(ref, rows, value, first=0):
    for c in range(value.shape[1] // 128):
        ref[first + c, rows, :] = value[:, 128 * c : 128 * (c + 1)]


def get(ref, rows):
    return jnp.concatenate([ref[c, rows, :] for c in range(ref.shape[0])], axis=1)


def lanes(shape):
    return lax.broadcasted_iota(jnp.int32, shape, len(shape) - 1)


def rotate(vector, table):
    lower = lanes(vector.shape) % 64 < 32
    partner = jnp.where(lower, pltpu.roll(vector, 96, 1), pltpu.roll(vector, 32, 1))
    return vector * table[0:1, :] + partner * table[1:2, :]


def rotation_table(position):
    frequency = THETA ** (-np.arange(32, dtype=np.float64) / 32)
    angles = position * frequency
    cos, sin = np.cos(angles), np.sin(angles)
    return np.stack(
        [np.tile(np.concatenate([cos, cos]), 2), np.tile(np.concatenate([-sin, sin]), 2)]
    ).astype(np.float32)


INPUTS = (
    "resid",
    "attn_gain",
    "post_gain",
    "mlp_gain",
    "latent_gain",
    "table",
    "wqn",
    "wqr",
    "wl",
    "wkr",
    "ku",
    "vu",
    "wo",
    "wg",
    "wu",
    "wd",
    "cl",
    "cr",
)


def kernel(n_kv, n_tp, *refs):
    n_in = len(INPUTS)
    hbm = dict(zip(INPUTS, refs[:n_in]))
    out = refs[n_in]
    scratch = refs[n_in + 1 :]
    v = dict(zip(INPUTS, scratch[:n_in]))
    (
        load_sem,
        f1, sb_l, rb_l, rb1, f2, sb2, rb2, f3, sb3, rb3, fq, rb_q, sb4, rb4, f5, sb5, rb5, fo, rb6,
        f7, sb7, rb7, sb8, rb8, mid, rb9, f10, sb10, rb10, sb11, rb11, rb12, sb12, g1, nl, pairs, up_k, up_v,
        tp_send, tp_recv, kv_send, kv_recv, q_recv, o_recv,
    ) = scratch[n_in:]

    k, t = lax.axis_index("kv"), lax.axis_index("tp")
    own = v["resid"].shape[0]
    batch = own * n_tp
    width = v["resid"].shape[1]
    model = width * n_kv
    lat = v["cl"].shape[2]
    quarters = n_kv // own
    share = batch // n_kv
    heads = 2 * n_tp
    heads_q = heads // quarters
    tp_q = n_tp // quarters
    ff = v["wg"].shape[0]
    scale = (128 + 64) ** (-0.5)
    slot, group = lax.rem(k, own), lax.div(k, own)

    def far_tp(i):
        return lax.rem(t + n_tp // 2 + lax.div(i + 1, 2) * (1 - 2 * lax.rem(i, 2)) + n_tp, n_tp)

    rows_kv = n_kv // own
    steps = [(y, x) for y in range(rows_kv) for x in range(own) if (y, x) != (0, 0)]
    steps.sort(key=lambda step: -min(step[0], rows_kv - step[0]) - min(step[1], own - step[1]))
    far_kv = [lax.rem(group + y, rows_kv) * own + lax.rem(slot + x, own) for y, x in steps]

    barrier = pltpu.get_barrier_semaphore()

    @pl.loop(0, n_tp - 1)
    def _(i):
        pl.semaphore_signal(barrier, inc=1, device_id={"kv": k, "tp": far_tp(i)}, device_id_type=MESH)

    for to in far_kv:
        pl.semaphore_signal(barrier, inc=1, device_id={"kv": to, "tp": t}, device_id_type=MESH)

    loads = {}
    for at, name in enumerate(INPUTS):
        source = hbm[name]
        if name == "wkr":
            source = source.at[:, pl.ds(pl.multiple_of(k * width, width), width)]
        loads[name] = pltpu.make_async_copy(source, v[name], load_sem.at[at])
        loads[name].start()

    def send(src, dst, send_sem, recv_sem, kv, tp):
        pltpu.make_async_remote_copy(
            src_ref=src,
            dst_ref=dst,
            send_sem=send_sem,
            recv_sem=recv_sem,
            device_id={"kv": kv, "tp": tp},
            device_id_type=MESH,
        ).start()

    def over_tp(src_of, dst, phase):
        @pl.loop(0, n_tp - 1)
        def _(i):
            to = far_tp(i)
            send(src_of(to), dst, tp_send.at[phase], tp_recv.at[phase], k, to)

    def over_kv(src_of, dst, phase, recv=None):
        for to in far_kv:
            send(src_of(to), dst, kv_send.at[phase], kv_recv.at[phase] if recv is None else recv, to, t)

    def by_head(name, to):
        @pl.loop(0, lat, unroll=16)
        def _(c):
            pairs[pl.ds(2 * c, 2), :] = v[name][c].astype(F32)

        for h in range(2):
            to[h] = pairs[pl.ds(h, lat, stride=2), :].astype(BF16)

    def take(ref, sem):
        pltpu.make_async_copy(ref, ref, sem).wait()

    def take_tp(ref, phase):
        take(ref.at[pl.ds(0, n_tp - 1)], tp_recv.at[phase])

    def take_kv(ref, phase):
        take(ref.at[pl.ds(0, n_kv - 1)], kv_recv.at[phase])

    for name in ("attn_gain", "post_gain", "mlp_gain", "resid", "wl", "wkr", "latent_gain", "table"):
        loads[name].wait()

    def block_of(name):
        g1[...] = v[name][...].astype(F32)
        per = width // 128
        return jnp.concatenate([g1[pl.ds(k * per + j, 1), :] for j in range(per)], axis=1)

    attn_gain, post_gain, mlp_gain = block_of("attn_gain"), block_of("post_gain"), block_of("mlp_gain")
    resid = v["resid"][...].astype(F32)
    own_normed = (resid * attn_gain).astype(BF16)
    sb_l[:, 0:lat] = dot(own_normed, v["wl"][...])
    key_part = dot(own_normed, v["wkr"][...], NT)
    square = jnp.sum(resid * resid, axis=1, keepdims=True)
    sb_l[:, lat : lat + 128] = jnp.concatenate([key_part, jnp.broadcast_to(square, (own, 64))], axis=1)

    pl.semaphore_wait(barrier, n_tp + n_kv - 2)

    over_tp(lambda to: v["resid"], rb1.at[t], 0)
    over_kv(lambda to: sb_l, rb_l.at[k], 0)
    rb1[t] = v["resid"][...]
    rb_l[k] = sb_l[...]
    for name in INPUTS:
        if name in ("wqn", "wqr", "ku", "vu", "wo", "wg", "wu", "wd"):
            loads[name].wait()
    by_head("ku", up_k)
    take_tp(rb1, 0)
    for j in range(n_tp):
        f1[own * j : own * (j + 1), :] = rb1[j].astype(F32)
    rows = f1[...]
    normed = (rows * attn_gain).astype(BF16)
    high, low = halves(jnp.sum(rows * rows, axis=1, keepdims=True))
    qw = v["wqn"].shape[1]
    every = slice(None)
    put(f2, every, dot(normed, v["wqn"][...]))
    put(f2, every, dot(normed, v["wqr"][...]), qw // 128)
    put(f2, every, jnp.where(lanes((batch, 128)) < 64, high, low), qw // 128 + 1)
    for j in range(n_kv):
        sb2[j] = get(f2, pl.ds(j, share, stride=n_kv)).astype(BF16)
    over_kv(lambda to: sb2.at[to], rb2.at[k], 1)
    rb2[k] = sb2[k]

    take_kv(rb_l, 0)
    total = rb_l[0]
    for j in range(1, n_kv):
        total = total + rb_l[j]
    latent = total[:, 0:lat]
    gain_rows = v["latent_gain"][...].astype(F32)
    latent_gain = jnp.concatenate([gain_rows[j : j + 1, :] for j in range(lat // 128)], axis=1)
    new_latent = (
        latent * lax.rsqrt(jnp.mean(latent * latent, axis=1, keepdims=True) + EPS) * latent_gain
    ).astype(BF16)
    out[:, width : width + lat] = new_latent.astype(F32)
    key = total[:, lat : lat + 128]
    own_scale = lax.rsqrt(key[:, 64:65] / model + EPS)
    table = v["table"][...]
    new_key = rotate(key * own_scale, table).astype(BF16)
    out[:, width + lat : width + lat + 128] = new_key.astype(F32)
    nl[:, 0:lat] = new_latent.astype(F32)
    nl[:, lat : lat + 128] = jnp.where(lanes((own, 128)) < 64, new_key.astype(F32), 0.0)

    take_kv(rb2, 1)
    total = rb2[0].astype(F32)
    for j in range(1, n_kv):
        total = total + rb2[j].astype(F32)
    squares = total[:, qw + 128 : qw + 129] + total[:, qw + 192 : qw + 193]
    scale_in = lax.rsqrt(squares / model + EPS)
    q_nope = (total[:, 0:qw] * scale_in).astype(BF16)
    q_rope = rotate(total[:, qw : qw + 128] * scale_in, table)
    for h in range(2):
        spot = pl.ds(h, share, stride=2)
        put(f3, spot, dot(q_nope[:, 128 * h : 128 * (h + 1)], up_k[h], NT))
        turned = q_rope if h == 0 else pltpu.roll(q_rope, 64, 1)
        put(f3, spot, jnp.where(lanes((share, 128)) < 64, turned, 0.0), lat // 128)
    for i in range(share):
        sb3[i] = get(f3, slice(2 * i, 2 * i + 2)).astype(BF16)
    @pl.loop(0, share)
    def _(i):
        to = quarters * i + group

        @pl.when(to != t)
        def _():
            send(sb3.at[i], rb3.at[t], tp_send.at[1], tp_recv.at[1], k, to)

        @pl.when(to == t)
        def _():
            rb3[t] = sb3[i]

    by_head("vu", up_v)
    gathers_q = lax.rem(t, quarters) == group

    @pl.when(gathers_q)
    def _():
        take_tp(rb3, 1)
        for j in range(n_tp):
            fq[2 * j : 2 * j + 2, :] = rb3[j].astype(F32)
        rb_q[slot] = fq[...].astype(BF16)
        over_kv(lambda to: rb_q.at[slot], rb_q.at[slot], 2, q_recv.at[slot])

    loads["cl"].wait()
    loads["cr"].wait()
    for s in range(own):
        @pl.when(k != own * lax.rem(t, quarters) + s)
        def _():
            take(rb_q.at[s], q_recv.at[s])

        keys = v["cl"][s]
        scores = (dot(rb_q[s, :, 0:lat], keys, NT) + dot(rb_q[s, :, lat : lat + 64], v["cr"][s])) * scale
        peak_high, peak_low = halves(jnp.max(scores, axis=1, keepdims=True))
        probs = jnp.exp(scores - (peak_high + peak_low))
        sum_high, sum_low = halves(jnp.sum(probs, axis=1, keepdims=True))
        sb4[s, :, 0:lat] = dot(probs.astype(BF16), keys).astype(BF16)
        lane = lanes((heads, 128))
        sb4[s, :, lat : lat + 128] = jnp.where(
            lane < 32, peak_high, jnp.where(lane < 64, peak_low, jnp.where(lane < 96, sum_high, sum_low))
        ).astype(BF16)
        for q in range(quarters):
            to = own * q + s

            @pl.when(k != to)
            def _():
                send(sb4.at[s, pl.ds(heads_q * q, heads_q)], rb4.at[k], kv_send.at[3], kv_recv.at[3], to, t)

            @pl.when(k == to)
            def _():
                rb4[k] = sb4[s, heads_q * q : heads_q * (q + 1), :]

    query = rb_q[slot, pl.ds(pl.multiple_of(group * heads_q, heads_q), heads_q), :].astype(F32)
    mine = nl[pl.ds(slot, 1), :]
    own_score = jnp.sum(query * mine, axis=1, keepdims=True) * scale
    take_kv(rb4, 3)
    peaks, sums = [], []
    top = own_score
    for j in range(n_kv):
        stats = rb4[j, :, lat : lat + 128].astype(F32)
        peaks.append(stats[:, 0:1] + stats[:, 32:33])
        sums.append(stats[:, 64:65] + stats[:, 96:97])
        top = jnp.maximum(top, peaks[-1])
    own_prob = jnp.exp(own_score - top)
    totals = own_prob
    summed = own_prob * mine[:, 0:lat]
    for j in range(n_kv):
        weight = jnp.exp(peaks[j] - top)
        totals = totals + sums[j] * weight
        summed = summed + rb4[j, :, 0:lat].astype(F32) * weight
    f5[...] = summed / totals
    for i in range(tp_q):
        sb5[i] = f5[2 * i : 2 * i + 2, :].astype(BF16)

    @pl.loop(0, tp_q)
    def _(i):
        to = tp_q * group + i

        @pl.when(to != t)
        def _():
            send(sb5.at[i], rb5.at[t], tp_send.at[2], tp_recv.at[2], k, to)

        @pl.when(to == t)
        def _():
            rb5[t] = sb5[i]

    gathers_o = lax.div(t, tp_q) == group

    @pl.when(gathers_o)
    def _():
        take_tp(rb5, 2)
        for j in range(n_tp):
            put(fo, slice(2 * j, 2 * j + 2), rb5[j].astype(F32))
        terms = [dot(get(fo, pl.ds(h, n_tp, stride=2)).astype(BF16), up_v[h]).astype(BF16) for h in range(2)]
        rb6[slot] = jnp.concatenate(terms, axis=1)
        over_kv(lambda to: rb6.at[slot], rb6.at[slot], 4, o_recv.at[slot])

    for s in range(own):
        @pl.when(k != own * lax.div(t, tp_q) + s)
        def _():
            take(rb6.at[s], o_recv.at[s])

        put(f7, slice(n_tp * s, n_tp * (s + 1)), dot(rb6[s], v["wo"][...]))
    for j in range(n_tp):
        sb7[j] = get(f7, pl.ds(j, own, stride=n_tp)).astype(BF16)
    over_tp(lambda to: sb7.at[to], rb7.at[t], 3)
    rb7[t] = sb7[t]
    take_tp(rb7, 3)
    attended = jnp.sum(rb7[...].astype(F32), axis=0)
    sb8[...] = jnp.broadcast_to(jnp.sum(attended * attended, axis=1, keepdims=True), sb8.shape)
    over_kv(lambda to: sb8, rb8.at[k], 5)
    rb8[k] = sb8[...]
    take_kv(rb8, 5)
    post_square = jnp.sum(rb8[...], axis=0)[:, 0:1]
    mid[...] = (resid + attended * lax.rsqrt(post_square / model + EPS) * post_gain).astype(BF16)
    over_tp(lambda to: mid, rb9.at[t], 4)
    rb9[t] = mid[...]
    take_tp(rb9, 4)
    for j in range(n_tp):
        f1[own * j : own * (j + 1), :] = rb9[j].astype(F32)
    rows = f1[...]
    normed = (rows * mlp_gain).astype(BF16)
    high, low = halves(jnp.sum(rows * rows, axis=1, keepdims=True))
    padded = -(-ff // 128) * 128
    free = padded - ff
    f10[:, padded - 128 : padded] = jnp.where(lanes((batch, 128)) < 128 - free // 2, high, low)
    f10[:, 2 * padded - 128 : 2 * padded] = jnp.zeros((batch, 128), F32)
    f10[:, 0:ff] = dot(normed, v["wg"][...], NT)
    f10[:, padded : padded + ff] = dot(normed, v["wu"][...], NT)
    for j in range(n_kv):
        sb10[j] = f10[share * j : share * (j + 1), :].astype(BF16)
    over_kv(lambda to: sb10.at[to], rb10.at[k], 6)
    rb10[k] = sb10[k]
    take_kv(rb10, 6)
    total = rb10[0].astype(F32)
    for j in range(1, n_kv):
        total = total + rb10[j].astype(F32)
    squares = total[:, ff : ff + 1] + total[:, padded - 1 : padded]
    scale_mid = lax.rsqrt(squares / model + EPS)
    gate, up = total[:, 0:padded] * scale_mid, total[:, padded : 2 * padded] * scale_mid
    hidden = gate / (1.0 + jnp.exp(-gate)) * up
    sb11[...] = jnp.where(lanes((share, padded)) < ff, hidden, 0.0).astype(BF16)
    over_kv(lambda to: sb11, rb11.at[k], 7)
    rb11[k] = sb11[...]
    take_kv(rb11, 7)
    everything = rb11[...].astype(F32).reshape(batch, padded).astype(BF16)
    f1[...] = dot(everything[:, 0:ff], v["wd"][...])
    for j in range(n_tp):
        sb12[j] = f1[own * j : own * (j + 1), :].astype(BF16)
    over_tp(lambda to: sb12.at[to], rb12.at[t], 5)
    rb12[t] = sb12[t]
    take_tp(rb12, 5)
    out[:, 0:width] = mid[...].astype(F32) + jnp.sum(rb12[...].astype(F32), axis=0)

    for phase, ref in ((0, rb1), (3, rb7), (4, rb9), (5, rb12)):
        take(ref.at[pl.ds(0, n_tp - 1)], tp_send.at[phase])
    for phase, ref in ((0, rb_l), (1, rb2), (3, rb4), (5, rb8), (6, rb10), (7, rb11)):
        take(ref.at[pl.ds(0, n_kv - 1)], kv_send.at[phase])
    for phase, ref, count, inside in ((1, rb3, share, gathers_q), (2, rb5, tp_q, gathers_o)):
        @pl.when(inside)
        def _():
            take(ref.at[pl.ds(0, count - 1)], tp_send.at[phase])

        @pl.when(jnp.logical_not(inside))
        def _():
            take(ref.at[pl.ds(0, count)], tp_send.at[phase])

    for phase, ref, inside in ((2, rb_q, gathers_q), (4, rb6, gathers_o)):
        @pl.when(inside)
        def _():
            @pl.loop(1, n_kv)
            def _(i):
                take(ref.at[0], kv_send.at[phase])


def split(parts, whole, *outs):
    for (start, size), out in zip(parts, outs):
        out[...] = whole[:, start : start + size].astype(BF16)


def body(
    resid, attn_gain, w_query_nope, w_query_rope, w_latent, w_key_rope, latent_gain, key_up, value_up,
    w_out, post_gain, mlp_gain, w_gate, w_up, w_down, cache_latent, cache_rope_key,
):
    n_kv, n_tp = lax.axis_size("kv"), lax.axis_size("tp")
    own, width = resid.shape
    batch, share = own * n_tp, own * n_tp // n_kv
    lat, positions = cache_latent.shape[2], cache_latent.shape[1]
    quarters = n_kv // own
    heads = 2 * n_tp
    heads_q, tp_q = heads // quarters, n_tp // quarters
    ff = w_gate.shape[1]
    padded = -(-ff // 128) * 128
    qw = w_query_nope.shape[1]
    operands = (
        resid,
        attn_gain.reshape(-1, 128),
        post_gain.reshape(-1, 128),
        mlp_gain.reshape(-1, 128),
        latent_gain.reshape(-1, 128),
        jnp.asarray(rotation_table(positions * n_kv)),
        w_query_nope,
        w_query_rope,
        w_latent,
        w_key_rope.T,
        key_up,
        value_up,
        w_out,
        w_gate.T,
        w_up.T,
        w_down,
        cache_latent,
        cache_rope_key.swapaxes(1, 2),
    )
    local = [pltpu.VMEM(o.shape, o.dtype) for o in operands]
    local[9] = pltpu.VMEM((64, width), BF16)
    wide = lat + 128
    dma = pltpu.SemaphoreType.DMA
    scratch = local + [
        dma((len(INPUTS),)),
        pltpu.VMEM((batch, width), F32),
        pltpu.VMEM((own, wide), F32),
        pltpu.VMEM((n_kv, own, wide), F32),
        pltpu.VMEM((n_tp, own, width), BF16),
        pltpu.VMEM((qw // 128 + 2, batch, 128), F32),
        pltpu.VMEM((n_kv, share, qw + 256), BF16),
        pltpu.VMEM((n_kv, share, qw + 256), BF16),
        pltpu.VMEM((wide // 128, 2 * share, 128), F32),
        pltpu.VMEM((share, 2, wide), BF16),
        pltpu.VMEM((n_tp, 2, wide), BF16),
        pltpu.VMEM((heads, wide), F32),
        pltpu.VMEM((own, heads, wide), BF16),
        pltpu.VMEM((own, heads, wide), BF16),
        pltpu.VMEM((n_kv, heads_q, wide), BF16),
        pltpu.VMEM((heads_q, lat), F32),
        pltpu.VMEM((tp_q, 2, lat), BF16),
        pltpu.VMEM((n_tp, 2, lat), BF16),
        pltpu.VMEM((lat // 128, heads, 128), F32),
        pltpu.VMEM((own, n_tp, 256), BF16),
        pltpu.VMEM((width // 128, batch, 128), F32),
        pltpu.VMEM((n_tp, own, width), BF16),
        pltpu.VMEM((n_tp, own, width), BF16),
        pltpu.VMEM((own, 128), F32),
        pltpu.VMEM((n_kv, own, 128), F32),
        pltpu.VMEM((own, width), BF16),
        pltpu.VMEM((n_tp, own, width), BF16),
        pltpu.VMEM((batch, 2 * padded), F32),
        pltpu.VMEM((n_kv, share, 2 * padded), BF16),
        pltpu.VMEM((n_kv, share, 2 * padded), BF16),
        pltpu.VMEM((share, padded), BF16),
        pltpu.VMEM((n_kv, share, padded), BF16),
        pltpu.VMEM((n_tp, own, width), BF16),
        pltpu.VMEM((n_tp, own, width), BF16),
        pltpu.VMEM((attn_gain.shape[0] // 128, 128), F32),
        pltpu.VMEM((own, wide), F32),
        pltpu.VMEM((2 * lat, 128), F32),
        pltpu.VMEM((2, lat, 128), BF16),
        pltpu.VMEM((2, lat, 128), BF16),
        dma((6,)),
        dma((6,)),
        dma((8,)),
        dma((8,)),
        dma((own,)),
        dma((own,)),
    ]
    out = pl.pallas_call(
        functools.partial(kernel, n_kv, n_tp),
        out_shape=jax.ShapeDtypeStruct((own, width + wide), F32),
        in_specs=[pl.BlockSpec(memory_space=pl.ANY)] * len(operands),
        out_specs=pl.BlockSpec(memory_space=pltpu.VMEM),
        scratch_shapes=scratch,
        compiler_params=pltpu.CompilerParams(
            collective_id=0, has_side_effects=True, vmem_limit_bytes=67043328
        ),
    )(*operands)
    parts = ((0, width), (width, lat), (width + lat, 64))
    return pl.pallas_call(
        functools.partial(split, parts),
        out_shape=tuple(jax.ShapeDtypeStruct((own, size), BF16) for _, size in parts),
        in_specs=[pl.BlockSpec(memory_space=pltpu.VMEM)],
        out_specs=(pl.BlockSpec(memory_space=pltpu.VMEM),) * 3,
    )(out)


def solution(mesh):
    placed = (
        P("tp", "kv"),
        P(),
        P("kv", "tp"),
        P("kv", "tp"),
        P("kv", None),
        P(),
        P(),
        P(None, "tp", None),
        P(None, "tp", None),
        P("tp", "kv"),
        P(),
        P(),
        P("kv", "tp"),
        P("kv", "tp"),
        P("tp", "kv"),
        P("tp", "kv", None),
        P("tp", "kv", None),
    )
    return jax.shard_map(
        body,
        mesh=mesh,
        in_specs=placed,
        out_specs=(P("tp", "kv"), P("tp", None), P("tp", None)),
        check_vma=False,
    )
```

```python
import functools

import jax
import jax.numpy as jnp
import numpy as np
from jax import lax
from jax.experimental import pallas as pl
from jax.experimental.pallas import tpu as pltpu
from jax.sharding import PartitionSpec as P

EPS = 1e-06
THETA = 10000.0
MESH = pl.DeviceIdType.MESH
F32 = jnp.float32
BF16 = jnp.bfloat16
NN = (((1,), (0,)), ((), ()))
NT = (((1,), (1,)), ((), ()))


def dot(a, b, dims=NN):
    return lax.dot_general(a, b, dims, preferred_element_type=F32)


def halves(value):
    high = value.astype(BF16).astype(F32)
    return high, (value - high).astype(BF16).astype(F32)


def put(ref, rows, value, first=0):
    for c in range(value.shape[1] // 128):
        ref[first + c, rows, :] = value[:, 128 * c : 128 * (c + 1)]


def get(ref, rows):
    return jnp.concatenate([ref[c, rows, :] for c in range(ref.shape[0])], axis=1)


def lanes(shape):
    return lax.broadcasted_iota(jnp.int32, shape, len(shape) - 1)


def rotate(vector, table):
    lower = lanes(vector.shape) % 64 < 32
    partner = jnp.where(lower, pltpu.roll(vector, 96, 1), pltpu.roll(vector, 32, 1))
    return vector * table[0:1, :] + partner * table[1:2, :]


def rotation_table(position):
    frequency = THETA ** (-np.arange(32, dtype=np.float64) / 32)
    angles = position * frequency
    cos, sin = np.cos(angles), np.sin(angles)
    return np.stack(
        [np.tile(np.concatenate([cos, cos]), 2), np.tile(np.concatenate([-sin, sin]), 2)]
    ).astype(np.float32)


INPUTS = (
    "resid",
    "attn_gain",
    "post_gain",
    "mlp_gain",
    "latent_gain",
    "table",
    "wqn",
    "wqr",
    "wl",
    "wkr",
    "ku",
    "vu",
    "wo",
    "wg",
    "wu",
    "wd",
    "cl",
    "cr",
)


def kernel(n_kv, n_tp, *refs):
    n_in = len(INPUTS)
    hbm = dict(zip(INPUTS, refs[:n_in]))
    out = refs[n_in]
    scratch = refs[n_in + 1 :]
    v = dict(zip(INPUTS, scratch[:n_in]))
    (
        load_sem,
        f1, sb_l, rb_l, rb1, f2, sb2, rb2, f3, sb3, rb3, fq, rb_q, sb4, rb4, f5, sb5, rb5, fo, rb6,
        f7, sb7, rb7, sb8, rb8, mid, rb9, f10, sb10, rb10, sb_r, rb_r, sum_r, f2r, sb11, rb11, rb12, sb12, g1, nl, pairs, up_k, up_v,
        tp_send, tp_recv, kv_send, kv_recv, q_recv, o_recv,
    ) = scratch[n_in:]

    k, t = lax.axis_index("kv"), lax.axis_index("tp")
    own = v["resid"].shape[0]
    batch = own * n_tp
    width = v["resid"].shape[1]
    model = width * n_kv
    lat = v["cl"].shape[2]
    quarters = n_kv // own
    share = batch // n_kv
    heads = 2 * n_tp
    heads_q = heads // quarters
    tp_q = n_tp // quarters
    ff = v["wg"].shape[0]
    scale = (128 + 64) ** (-0.5)
    padded = -(-ff // 128) * 128
    free = padded - ff
    lane_row = lanes((batch, 128))
    slot, group = lax.rem(k, own), lax.div(k, own)

    around = [n_tp // 2 + (i + 1) // 2 * (1 - 2 * (i % 2)) for i in range(n_tp - 1)]
    far_tp = [lax.rem(t + offset, n_tp) for offset in around]
    rows_kv = n_kv // own
    steps = [(y, x) for y in range(rows_kv) for x in range(own) if (y, x) != (0, 0)]
    steps.sort(key=lambda step: -min(step[0], rows_kv - step[0]) - min(step[1], own - step[1]))
    far_kv = [lax.rem(group + y, rows_kv) * own + lax.rem(slot + x, own) for y, x in steps]

    first = pltpu.make_async_copy(hbm["resid"], v["resid"], load_sem.at[0])
    first.start()
    barrier = pltpu.get_barrier_semaphore()

    for to in far_tp:
        pl.semaphore_signal(barrier, inc=1, device_id={"kv": k, "tp": to}, device_id_type=MESH)
    for to in far_kv:
        pl.semaphore_signal(barrier, inc=1, device_id={"kv": to, "tp": t}, device_id_type=MESH)

    loads = {}
    for at, name in enumerate(INPUTS):
        source = hbm[name]
        if name == "wkr":
            source = source.at[:, pl.ds(pl.multiple_of(k * width, width), width)]
        loads[name] = first if name == "resid" else pltpu.make_async_copy(source, v[name], load_sem.at[at])
        if name != "resid":
            loads[name].start()

    def send(src, dst, send_sem, recv_sem, kv, tp):
        pltpu.make_async_remote_copy(
            src_ref=src,
            dst_ref=dst,
            send_sem=send_sem,
            recv_sem=recv_sem,
            device_id={"kv": kv, "tp": tp},
            device_id_type=MESH,
        ).start()

    def over_tp(src_of, dst, phase):
        for to in far_tp:
            send(src_of(to), dst, tp_send.at[phase], tp_recv.at[phase], k, to)

    def over_kv(src_of, dst, phase, recv=None):
        for to in far_kv:
            send(src_of(to), dst, kv_send.at[phase], kv_recv.at[phase] if recv is None else recv, to, t)

    def by_head(name, to):
        @pl.loop(0, lat, unroll=16)
        def _(c):
            pairs[pl.ds(2 * c, 2), :] = v[name][c].astype(F32)

        for h in range(2):
            to[h] = pairs[pl.ds(h, lat, stride=2), :].astype(BF16)

    def gate_up(rows):
        f10[:, 2 * padded - 128 : 2 * padded] = jnp.zeros((batch, 128), F32)
        f10[:, 0:ff] = dot(rows, v["wg"][...], NT)
        f10[:, padded : padded + ff] = dot(rows, v["wu"][...], NT)

    def take(ref, sem):
        pltpu.make_async_copy(ref, ref, sem).wait()

    def take_tp(ref, phase):
        take(ref.at[pl.ds(0, n_tp - 1)], tp_recv.at[phase])

    def take_kv(ref, phase):
        take(ref.at[pl.ds(0, n_kv - 1)], kv_recv.at[phase])

    first.wait()
    pl.semaphore_wait(barrier, n_tp + n_kv - 2)

    over_tp(lambda to: v["resid"], rb1.at[t], 0)
    rb1[t] = v["resid"][...]
    for name in ("attn_gain", "post_gain", "mlp_gain", "wl", "wkr", "latent_gain", "table"):
        loads[name].wait()

    def block_of(name):
        g1[...] = v[name][...].astype(F32)
        per = width // 128
        return jnp.concatenate([g1[pl.ds(k * per + j, 1), :] for j in range(per)], axis=1)

    attn_gain, post_gain, mlp_gain = block_of("attn_gain"), block_of("post_gain"), block_of("mlp_gain")
    resid = v["resid"][...].astype(F32)
    own_normed = (resid * attn_gain).astype(BF16)
    sb_l[:, 0:lat] = dot(own_normed, v["wl"][...])
    key_part = dot(own_normed, v["wkr"][...], NT)
    square = jnp.sum(resid * resid, axis=1, keepdims=True)
    sb_l[:, lat : lat + 128] = jnp.concatenate([key_part, jnp.broadcast_to(square, (own, 64))], axis=1)
    over_kv(lambda to: sb_l, rb_l.at[k], 0)
    rb_l[k] = sb_l[...]
    for name in INPUTS:
        if name in ("wqn", "wqr", "ku", "vu", "wo", "wg", "wu", "wd"):
            loads[name].wait()
    by_head("ku", up_k)
    take_tp(rb1, 0)
    for j in range(n_tp):
        f1[own * j : own * (j + 1), :] = rb1[j].astype(F32)
    rows = f1[...]
    normed = (rows * attn_gain).astype(BF16)
    high, low = halves(jnp.sum(rows * rows, axis=1, keepdims=True))
    qw = v["wqn"].shape[1]
    every = slice(None)
    put(f2, every, dot(normed, v["wqn"][...]))
    put(f2, every, dot(normed, v["wqr"][...]), qw // 128)
    put(f2, every, jnp.where(lanes((batch, 128)) < 64, high, low), qw // 128 + 1)
    for j in range(n_kv):
        sb2[j] = get(f2, pl.ds(j, share, stride=n_kv)).astype(BF16)
    over_kv(lambda to: sb2.at[to], rb2.at[k], 1)
    rb2[k] = sb2[k]

    take_kv(rb_l, 0)
    total = rb_l[0]
    for j in range(1, n_kv):
        total = total + rb_l[j]
    latent = total[:, 0:lat]
    gain_rows = v["latent_gain"][...].astype(F32)
    latent_gain = jnp.concatenate([gain_rows[j : j + 1, :] for j in range(lat // 128)], axis=1)
    new_latent = (
        latent * lax.rsqrt(jnp.mean(latent * latent, axis=1, keepdims=True) + EPS) * latent_gain
    ).astype(BF16)
    out[:, width : width + lat] = new_latent.astype(F32)
    key = total[:, lat : lat + 128]
    own_scale = lax.rsqrt(key[:, 64:65] / model + EPS)
    table = v["table"][...]
    new_key = rotate(key * own_scale, table).astype(BF16)
    out[:, width + lat : width + lat + 128] = new_key.astype(F32)
    nl[:, 0:lat] = new_latent.astype(F32)
    nl[:, lat : lat + 128] = jnp.where(lanes((own, 128)) < 64, new_key.astype(F32), 0.0)

    take_kv(rb2, 1)
    total = rb2[0].astype(F32)
    for j in range(1, n_kv):
        total = total + rb2[j].astype(F32)
    squares = total[:, qw + 128 : qw + 129] + total[:, qw + 192 : qw + 193]
    scale_in = lax.rsqrt(squares / model + EPS)
    q_nope = (total[:, 0:qw] * scale_in).astype(BF16)
    q_rope = rotate(total[:, qw : qw + 128] * scale_in, table)
    for h in range(2):
        spot = pl.ds(h, share, stride=2)
        put(f3, spot, dot(q_nope[:, 128 * h : 128 * (h + 1)], up_k[h], NT))
        turned = q_rope if h == 0 else pltpu.roll(q_rope, 64, 1)
        put(f3, spot, jnp.where(lanes((share, 128)) < 64, turned, 0.0), lat // 128)
    for i in range(share):
        sb3[i] = get(f3, slice(2 * i, 2 * i + 2)).astype(BF16)
    line = lax.div(t, tp_q)
    place = lax.rem(t, tp_q)
    stays = jnp.logical_and(line == group, lax.rem(t, quarters) == group)

    @pl.loop(0, share)
    def _(i):
        to = quarters * i + group
        home = jnp.logical_and(to == t, line == group)

        @pl.when(jnp.logical_not(home))
        def _():
            send(sb3.at[i], rb3.at[place], tp_send.at[1], tp_recv.at[1], own * line + slot, to)

        @pl.when(home)
        def _():
            rb3[place] = sb3[i]

    by_head("vu", up_v)
    normed = (f1[...] * mlp_gain).astype(BF16)
    gate_up(normed)
    f10[:, padded - 128 : padded] = jnp.where(
        lane_row < 128 - free, f10[:, padded - 128 : padded], jnp.where(lane_row < 128 - free // 2, high, low)
    )
    for j in range(n_kv):
        sb_r[j] = f10[share * j : share * (j + 1), :].astype(BF16)
    over_kv(lambda to: sb_r.at[to], rb_r.at[k], 8)
    rb_r[k] = sb_r[k]

    @pl.when(stays)
    def _():
        take(rb3.at[pl.ds(0, tp_q - 1)], tp_recv.at[1])

    @pl.when(jnp.logical_not(stays))
    def _():
        take(rb3, tp_recv.at[1])

    for j in range(tp_q):
        fq[2 * j : 2 * j + 2, :] = rb3[j].astype(F32)
    part = pl.ds(pl.multiple_of(group * heads_q, heads_q), heads_q)
    rb_q[slot, part, :] = fq[...].astype(BF16)
    over_kv(lambda to: rb_q.at[slot, part], rb_q.at[slot, part], 2, q_recv.at[slot])

    loads["cl"].wait()
    loads["cr"].wait()
    for s in range(own):
        @pl.when(slot == s)
        def _():
            if quarters > 1:
                take(rb_q.at[s, pl.ds(0, heads_q * (quarters - 1))], q_recv.at[s])

        @pl.when(slot != s)
        def _():
            take(rb_q.at[s], q_recv.at[s])

        keys = v["cl"][s]
        scores = (dot(rb_q[s, :, 0:lat], keys, NT) + dot(rb_q[s, :, lat : lat + 64], v["cr"][s])) * scale
        peak_high, peak_low = halves(jnp.max(scores, axis=1, keepdims=True))
        probs = jnp.exp(scores - (peak_high + peak_low))
        sum_high, sum_low = halves(jnp.sum(probs, axis=1, keepdims=True))
        sb4[s, :, 0:lat] = dot(probs.astype(BF16), keys).astype(BF16)
        lane = lanes((heads, 128))
        sb4[s, :, lat : lat + 128] = jnp.where(
            lane < 32, peak_high, jnp.where(lane < 64, peak_low, jnp.where(lane < 96, sum_high, sum_low))
        ).astype(BF16)
        for q in range(quarters):
            to = own * q + s

            @pl.when(k != to)
            def _():
                send(sb4.at[s, pl.ds(heads_q * q, heads_q)], rb4.at[k], kv_send.at[3], kv_recv.at[3], to, t)

            @pl.when(k == to)
            def _():
                rb4[k] = sb4[s, heads_q * q : heads_q * (q + 1), :]

    query = rb_q[slot, part, :].astype(F32)
    mine = nl[pl.ds(slot, 1), :]
    own_score = jnp.sum(query * mine, axis=1, keepdims=True) * scale
    take_kv(rb4, 3)
    peaks, sums = [], []
    top = own_score
    for j in range(n_kv):
        stats = rb4[j, :, lat : lat + 128].astype(F32)
        peaks.append(stats[:, 0:1] + stats[:, 32:33])
        sums.append(stats[:, 64:65] + stats[:, 96:97])
        top = jnp.maximum(top, peaks[-1])
    own_prob = jnp.exp(own_score - top)
    totals = own_prob
    summed = own_prob * mine[:, 0:lat]
    for j in range(n_kv):
        weight = jnp.exp(peaks[j] - top)
        totals = totals + sums[j] * weight
        summed = summed + rb4[j, :, 0:lat].astype(F32) * weight
    f5[...] = summed / totals
    for i in range(tp_q):
        sb5[i] = f5[2 * i : 2 * i + 2, :].astype(BF16)

    @pl.loop(0, tp_q)
    def _(i):
        to = tp_q * group + i

        @pl.when(to != t)
        def _():
            send(sb5.at[i], rb5.at[t], tp_send.at[2], tp_recv.at[2], k, to)

        @pl.when(to == t)
        def _():
            rb5[t] = sb5[i]

    take_kv(rb_r, 8)
    total = rb_r[0].astype(F32)
    for j in range(1, n_kv):
        total = total + rb_r[j].astype(F32)
    sum_r[...] = total
    gathers_o = lax.div(t, tp_q) == group

    @pl.when(gathers_o)
    def _():
        take_tp(rb5, 2)
        for j in range(n_tp):
            put(fo, slice(2 * j, 2 * j + 2), rb5[j].astype(F32))
        terms = [dot(get(fo, pl.ds(h, n_tp, stride=2)).astype(BF16), up_v[h]).astype(BF16) for h in range(2)]
        rb6[slot] = jnp.concatenate(terms, axis=1)
        over_kv(lambda to: rb6.at[slot], rb6.at[slot], 4, o_recv.at[slot])

    for s in range(own):
        @pl.when(k != own * lax.div(t, tp_q) + s)
        def _():
            take(rb6.at[s], o_recv.at[s])

        put(f7, slice(n_tp * s, n_tp * (s + 1)), dot(rb6[s], v["wo"][...]))
    for j in range(n_tp):
        sb7[j] = get(f7, pl.ds(j, own, stride=n_tp)).astype(BF16)
    over_tp(lambda to: sb7.at[to], rb7.at[t], 3)
    rb7[t] = sb7[t]
    take_tp(rb7, 3)
    attended = jnp.sum(rb7[...].astype(F32), axis=0)
    sb8[...] = jnp.broadcast_to(jnp.sum(attended * attended, axis=1, keepdims=True), sb8.shape)
    over_kv(lambda to: sb8, rb8.at[k], 5)
    rb8[k] = sb8[...]
    mid[...] = attended.astype(BF16)
    over_tp(lambda to: mid, rb9.at[t], 4)
    rb9[t] = mid[...]
    take_tp(rb9, 4)
    for j in range(n_tp):
        f2r[own * j : own * (j + 1), :] = rb9[j].astype(F32)
    rows = f2r[...]
    post = rows * post_gain
    gate_up((post * mlp_gain).astype(BF16))
    stats = []
    for product in (rows * rows, f1[...] * post, post * post):
        stats.extend(halves(jnp.sum(product, axis=1, keepdims=True)))
    for at, picks in ((padded, stats[0:4]), (2 * padded, stats[4:6])):
        tile = f10[:, at - 128 : at]
        for n, pick in enumerate(picks):
            tile = jnp.where(lane_row >= 128 - free + n * (free // len(picks)), pick, tile)
        f10[:, at - 128 : at] = tile
    for j in range(n_kv):
        sb10[j] = f10[share * j : share * (j + 1), :].astype(BF16)
    over_kv(lambda to: sb10.at[to], rb10.at[k], 6)
    rb10[k] = sb10[k]
    take_kv(rb10, 6)
    total = rb10[0].astype(F32)
    for j in range(1, n_kv):
        total = total + rb10[j].astype(F32)
    base = sum_r[...]
    quarter = free // 4

    def stat(value, at, width):
        return value[:, at : at + 1] + value[:, at + width : at + width + 1]

    resid_square = stat(base, ff, free // 2)
    factor = lax.rsqrt(stat(total, ff, quarter) / model + EPS)
    mixed = stat(total, ff + 2 * quarter, quarter)
    post_sum = stat(total, padded + ff, free // 2)
    mid_square = jnp.maximum(resid_square + factor * (2.0 * mixed + factor * post_sum), 0.0)
    scale_mid = lax.rsqrt(mid_square / model + EPS)
    both = (base + factor * total) * scale_mid
    gate, up = both[:, 0:padded], both[:, padded : 2 * padded]
    hidden = gate / (1.0 + jnp.exp(-gate)) * up
    sb11[...] = jnp.where(lanes((share, padded)) < ff, hidden, 0.0).astype(BF16)
    over_kv(lambda to: sb11, rb11.at[k], 7)
    rb11[k] = sb11[...]
    take_kv(rb11, 7)
    everything = rb11[...].astype(F32).reshape(batch, padded).astype(BF16)
    f1[...] = dot(everything[:, 0:ff], v["wd"][...])
    for j in range(n_tp):
        sb12[j] = f1[own * j : own * (j + 1), :].astype(BF16)
    over_tp(lambda to: sb12.at[to], rb12.at[t], 5)
    rb12[t] = sb12[t]
    take_kv(rb8, 5)
    post_square = jnp.sum(rb8[...], axis=0)[:, 0:1]
    resid_mid = (resid + attended * lax.rsqrt(post_square / model + EPS) * post_gain).astype(BF16).astype(F32)
    take_tp(rb12, 5)
    out[:, 0:width] = resid_mid + jnp.sum(rb12[...].astype(F32), axis=0)

    for phase, ref in ((0, rb1), (3, rb7), (4, rb9), (5, rb12)):
        take(ref.at[pl.ds(0, n_tp - 1)], tp_send.at[phase])
    for phase, ref in ((0, rb_l), (1, rb2), (3, rb4), (5, rb8), (6, rb10), (7, rb11), (8, rb_r)):
        take(ref.at[pl.ds(0, n_kv - 1)], kv_send.at[phase])
    for phase, ref, count, inside in ((1, sb3, share, stays), (2, rb5, tp_q, gathers_o)):
        @pl.when(inside)
        def _():
            take(ref.at[pl.ds(0, count - 1)], tp_send.at[phase])

        @pl.when(jnp.logical_not(inside))
        def _():
            take(ref.at[pl.ds(0, count)], tp_send.at[phase])

    take(rb4.at[pl.ds(0, n_kv - 1)], kv_send.at[2])

    @pl.when(gathers_o)
    def _():
        @pl.loop(1, n_kv)
        def _(i):
            take(rb6.at[0], kv_send.at[4])


def split(parts, whole, *outs):
    for (start, size), out in zip(parts, outs):
        out[...] = whole[:, start : start + size].astype(BF16)


def body(
    resid, attn_gain, w_query_nope, w_query_rope, w_latent, w_key_rope, latent_gain, key_up, value_up,
    w_out, post_gain, mlp_gain, w_gate, w_up, w_down, cache_latent, cache_rope_key,
):
    n_kv, n_tp = lax.axis_size("kv"), lax.axis_size("tp")
    own, width = resid.shape
    batch, share = own * n_tp, own * n_tp // n_kv
    lat, positions = cache_latent.shape[2], cache_latent.shape[1]
    quarters = n_kv // own
    heads = 2 * n_tp
    heads_q, tp_q = heads // quarters, n_tp // quarters
    ff = w_gate.shape[1]
    padded = -(-ff // 128) * 128
    qw = w_query_nope.shape[1]
    operands = (
        resid,
        attn_gain.reshape(-1, 128),
        post_gain.reshape(-1, 128),
        mlp_gain.reshape(-1, 128),
        latent_gain.reshape(-1, 128),
        jnp.asarray(rotation_table(positions * n_kv)),
        w_query_nope,
        w_query_rope,
        w_latent,
        w_key_rope.T,
        key_up,
        value_up,
        w_out,
        w_gate.T,
        w_up.T,
        w_down,
        cache_latent,
        cache_rope_key.swapaxes(1, 2),
    )
    local = [pltpu.VMEM(o.shape, o.dtype) for o in operands]
    local[9] = pltpu.VMEM((64, width), BF16)
    wide = lat + 128
    dma = pltpu.SemaphoreType.DMA
    scratch = local + [
        dma((len(INPUTS),)),
        pltpu.VMEM((batch, width), F32),
        pltpu.VMEM((own, wide), F32),
        pltpu.VMEM((n_kv, own, wide), F32),
        pltpu.VMEM((n_tp, own, width), BF16),
        pltpu.VMEM((qw // 128 + 2, batch, 128), F32),
        pltpu.VMEM((n_kv, share, qw + 256), BF16),
        pltpu.VMEM((n_kv, share, qw + 256), BF16),
        pltpu.VMEM((wide // 128, 2 * share, 128), F32),
        pltpu.VMEM((share, 2, wide), BF16),
        pltpu.VMEM((tp_q, 2, wide), BF16),
        pltpu.VMEM((heads_q, wide), F32),
        pltpu.VMEM((own, heads, wide), BF16),
        pltpu.VMEM((own, heads, wide), BF16),
        pltpu.VMEM((n_kv, heads_q, wide), BF16),
        pltpu.VMEM((heads_q, lat), F32),
        pltpu.VMEM((tp_q, 2, lat), BF16),
        pltpu.VMEM((n_tp, 2, lat), BF16),
        pltpu.VMEM((lat // 128, heads, 128), F32),
        pltpu.VMEM((own, n_tp, 256), BF16),
        pltpu.VMEM((width // 128, batch, 128), F32),
        pltpu.VMEM((n_tp, own, width), BF16),
        pltpu.VMEM((n_tp, own, width), BF16),
        pltpu.VMEM((own, 128), F32),
        pltpu.VMEM((n_kv, own, 128), F32),
        pltpu.VMEM((own, width), BF16),
        pltpu.VMEM((n_tp, own, width), BF16),
        pltpu.VMEM((batch, 2 * padded), F32),
        pltpu.VMEM((n_kv, share, 2 * padded), BF16),
        pltpu.VMEM((n_kv, share, 2 * padded), BF16),
        pltpu.VMEM((n_kv, share, 2 * padded), BF16),
        pltpu.VMEM((n_kv, share, 2 * padded), BF16),
        pltpu.VMEM((share, 2 * padded), F32),
        pltpu.VMEM((batch, width), F32),
        pltpu.VMEM((share, padded), BF16),
        pltpu.VMEM((n_kv, share, padded), BF16),
        pltpu.VMEM((n_tp, own, width), BF16),
        pltpu.VMEM((n_tp, own, width), BF16),
        pltpu.VMEM((attn_gain.shape[0] // 128, 128), F32),
        pltpu.VMEM((own, wide), F32),
        pltpu.VMEM((2 * lat, 128), F32),
        pltpu.VMEM((2, lat, 128), BF16),
        pltpu.VMEM((2, lat, 128), BF16),
        dma((6,)),
        dma((6,)),
        dma((9,)),
        dma((9,)),
        dma((own,)),
        dma((own,)),
    ]
    out = pl.pallas_call(
        functools.partial(kernel, n_kv, n_tp),
        out_shape=jax.ShapeDtypeStruct((own, width + wide), F32),
        in_specs=[pl.BlockSpec(memory_space=pl.ANY)] * len(operands),
        out_specs=pl.BlockSpec(memory_space=pltpu.VMEM),
        scratch_shapes=scratch,
        compiler_params=pltpu.CompilerParams(
            collective_id=0, has_side_effects=True, vmem_limit_bytes=67043328
        ),
    )(*operands)
    parts = ((0, width), (width, lat), (width + lat, 64))
    return pl.pallas_call(
        functools.partial(split, parts),
        out_shape=tuple(jax.ShapeDtypeStruct((own, size), BF16) for _, size in parts),
        in_specs=[pl.BlockSpec(memory_space=pltpu.VMEM)],
        out_specs=(pl.BlockSpec(memory_space=pltpu.VMEM),) * 3,
    )(out)


def solution(mesh):
    placed = (
        P("tp", "kv"),
        P(),
        P("kv", "tp"),
        P("kv", "tp"),
        P("kv", None),
        P(),
        P(),
        P(None, "tp", None),
        P(None, "tp", None),
        P("tp", "kv"),
        P(),
        P(),
        P("kv", "tp"),
        P("kv", "tp"),
        P("tp", "kv"),
        P("tp", "kv", None),
        P("tp", "kv", None),
    )
    return jax.shard_map(
        body,
        mesh=mesh,
        in_specs=placed,
        out_specs=(P("tp", "kv"), P("tp", None), P("tp", None)),
        check_vma=False,
    )
```

```python
import functools

import jax
import jax.numpy as jnp
import numpy as np
from jax import lax
from jax.experimental import pallas as pl
from jax.experimental.pallas import tpu as pltpu
from jax.sharding import PartitionSpec as P

EPS = 1e-06
THETA = 10000.0
MESH = pl.DeviceIdType.MESH
F32 = jnp.float32
BF16 = jnp.bfloat16
NN = (((1,), (0,)), ((), ()))
NT = (((1,), (1,)), ((), ()))


def dot(a, b, dims=NN):
    return lax.dot_general(a, b, dims, preferred_element_type=F32)


def halves(value):
    high = value.astype(BF16).astype(F32)
    return high, (value - high).astype(BF16).astype(F32)


def put(ref, rows, value, first=0):
    for c in range(value.shape[1] // 128):
        ref[first + c, rows, :] = value[:, 128 * c : 128 * (c + 1)]


def get(ref, rows):
    return jnp.concatenate([ref[c, rows, :] for c in range(ref.shape[0])], axis=1)


def lanes(shape):
    return lax.broadcasted_iota(jnp.int32, shape, len(shape) - 1)


def rotate(vector, table):
    lower = lanes(vector.shape) % 64 < 32
    partner = jnp.where(lower, pltpu.roll(vector, 96, 1), pltpu.roll(vector, 32, 1))
    return vector * table[0:1, :] + partner * table[1:2, :]


def rotation_table(position):
    frequency = THETA ** (-np.arange(32, dtype=np.float64) / 32)
    angles = position * frequency
    cos, sin = np.cos(angles), np.sin(angles)
    return np.stack(
        [np.tile(np.concatenate([cos, cos]), 2), np.tile(np.concatenate([-sin, sin]), 2)]
    ).astype(np.float32)


INPUTS = (
    "resid",
    "attn_gain",
    "post_gain",
    "mlp_gain",
    "latent_gain",
    "table",
    "wqn",
    "wqr",
    "wl",
    "wkr",
    "ku",
    "vu",
    "wo",
    "wg",
    "wu",
    "wd",
    "cl",
    "cr",
)


def kernel(n_kv, n_tp, *refs):
    n_in = len(INPUTS)
    hbm = dict(zip(INPUTS, refs[:n_in]))
    out = refs[n_in]
    scratch = refs[n_in + 1 :]
    v = dict(zip(INPUTS, scratch[:n_in]))
    (
        load_sem,
        f1, sb_l, rb_l, rb1, f2, sb2, rb2, f3, sb3, rb3, fq, rb_q, sb4, rb4, f5, sb5, rb5, fo, rb6,
        f7, sb7, rb7, sb8, rb8, mid, rb9, f10, sb10, rb10, sb_r, rb_r, sum_r, f2r, sb11, rb11, rb12, sb12, g1, nl, pairs, up_k, up_v, factors,
        tp_send, tp_recv, kv_send, kv_recv, q_recv, o_recv,
    ) = scratch[n_in:]

    k, t = lax.axis_index("kv"), lax.axis_index("tp")
    own = v["resid"].shape[0]
    batch = own * n_tp
    width = v["resid"].shape[1]
    model = width * n_kv
    lat = v["cl"].shape[2]
    quarters = n_kv // own
    share = batch // n_kv
    heads = 2 * n_tp
    heads_q = heads // quarters
    tp_q = n_tp // quarters
    ff = v["wg"].shape[0]
    scale = (128 + 64) ** (-0.5)
    padded = -(-ff // 128) * 128
    free = padded - ff
    lane_row = lanes((batch, 128))
    slot, group = lax.rem(k, own), lax.div(k, own)

    around = [n_tp // 2 + (i + 1) // 2 * (1 - 2 * (i % 2)) for i in range(n_tp - 1)]
    far_tp = [lax.rem(t + offset, n_tp) for offset in around]
    rows_kv = n_kv // own
    steps = [(y, x) for y in range(rows_kv) for x in range(own) if (y, x) != (0, 0)]
    steps.sort(key=lambda step: -min(step[0], rows_kv - step[0]) - min(step[1], own - step[1]))
    far_kv = [lax.rem(group + y, rows_kv) * own + lax.rem(slot + x, own) for y, x in steps]

    first = pltpu.make_async_copy(hbm["resid"], v["resid"], load_sem.at[0])
    first.start()
    barrier = pltpu.get_barrier_semaphore()

    for to in far_tp:
        pl.semaphore_signal(barrier, inc=1, device_id={"kv": k, "tp": to}, device_id_type=MESH)
    for to in far_kv:
        pl.semaphore_signal(barrier, inc=1, device_id={"kv": to, "tp": t}, device_id_type=MESH)

    loads = {}
    for at, name in enumerate(INPUTS):
        source = hbm[name]
        if name == "wkr":
            source = source.at[:, pl.ds(pl.multiple_of(k * width, width), width)]
        loads[name] = first if name == "resid" else pltpu.make_async_copy(source, v[name], load_sem.at[at])
        if name != "resid":
            loads[name].start()

    def send(src, dst, send_sem, recv_sem, kv, tp):
        pltpu.make_async_remote_copy(
            src_ref=src,
            dst_ref=dst,
            send_sem=send_sem,
            recv_sem=recv_sem,
            device_id={"kv": kv, "tp": tp},
            device_id_type=MESH,
        ).start()

    def over_tp(src_of, dst, phase):
        for to in far_tp:
            send(src_of(to), dst, tp_send.at[phase], tp_recv.at[phase], k, to)

    def over_kv(src_of, dst, phase, recv=None):
        for to in far_kv:
            send(src_of(to), dst, kv_send.at[phase], kv_recv.at[phase] if recv is None else recv, to, t)

    def by_head(name, to):
        @pl.loop(0, lat, unroll=16)
        def _(c):
            pairs[pl.ds(2 * c, 2), :] = v[name][c].astype(F32)

        for h in range(2):
            to[h] = pairs[pl.ds(h, lat, stride=2), :].astype(BF16)

    def gate_up(rows):
        f10[:, 2 * padded - 128 : 2 * padded] = jnp.zeros((batch, 128), F32)
        f10[:, 0:ff] = dot(rows, v["wg"][...], NT)
        f10[:, padded : padded + ff] = dot(rows, v["wu"][...], NT)

    def take(ref, sem):
        pltpu.make_async_copy(ref, ref, sem).wait()

    def take_tp(ref, phase):
        take(ref.at[pl.ds(0, n_tp - 1)], tp_recv.at[phase])

    def take_kv(ref, phase):
        take(ref.at[pl.ds(0, n_kv - 1)], kv_recv.at[phase])

    first.wait()
    pl.semaphore_wait(barrier, n_tp + n_kv - 2)

    over_tp(lambda to: v["resid"], rb1.at[t], 0)
    rb1[t] = v["resid"][...]
    for name in ("attn_gain", "post_gain", "mlp_gain", "wl", "wkr", "latent_gain", "table"):
        loads[name].wait()

    def block_of(name):
        g1[...] = v[name][...].astype(F32)
        per = width // 128
        return jnp.concatenate([g1[pl.ds(k * per + j, 1), :] for j in range(per)], axis=1)

    attn_gain, post_gain, mlp_gain = block_of("attn_gain"), block_of("post_gain"), block_of("mlp_gain")
    resid = v["resid"][...].astype(F32)
    own_normed = (resid * attn_gain).astype(BF16)
    sb_l[:, 0:lat] = dot(own_normed, v["wl"][...])
    key_part = dot(own_normed, v["wkr"][...], NT)
    square = jnp.sum(resid * resid, axis=1, keepdims=True)
    sb_l[:, lat : lat + 128] = jnp.concatenate([key_part, jnp.broadcast_to(square, (own, 64))], axis=1)
    over_kv(lambda to: sb_l, rb_l.at[k], 0)
    rb_l[k] = sb_l[...]
    for name in INPUTS:
        if name in ("wqn", "wqr", "ku", "vu", "wo", "wg", "wu", "wd"):
            loads[name].wait()
    by_head("ku", up_k)
    take_tp(rb1, 0)
    for j in range(n_tp):
        f1[own * j : own * (j + 1), :] = rb1[j].astype(F32)
    rows = f1[...]
    normed = (rows * attn_gain).astype(BF16)
    qw = v["wqn"].shape[1]
    every = slice(None)
    put(f2, every, dot(normed, v["wqn"][...]))
    put(f2, every, dot(normed, v["wqr"][...]), qw // 128)
    for j in range(n_kv):
        sb2[j] = get(f2, pl.ds(j, share, stride=n_kv)).astype(BF16)
    over_kv(lambda to: sb2.at[to], rb2.at[k], 1)
    rb2[k] = sb2[k]

    take_kv(rb_l, 0)
    total = rb_l[0]
    for j in range(1, n_kv):
        total = total + rb_l[j]
    latent = total[:, 0:lat]
    gain_rows = v["latent_gain"][...].astype(F32)
    latent_gain = jnp.concatenate([gain_rows[j : j + 1, :] for j in range(lat // 128)], axis=1)
    new_latent = (
        latent * lax.rsqrt(jnp.mean(latent * latent, axis=1, keepdims=True) + EPS) * latent_gain
    ).astype(BF16)
    out[:, width : width + lat] = new_latent.astype(F32)
    key = total[:, lat : lat + 128]
    own_scale = lax.rsqrt(key[:, 64:65] / model + EPS)
    table = v["table"][...]
    new_key = rotate(key * own_scale, table).astype(BF16)
    out[:, width + lat : width + lat + 128] = new_key.astype(F32)
    factors[...] = jnp.broadcast_to(own_scale * scale, factors.shape)
    nl[:, 0:lat] = new_latent.astype(F32)
    nl[:, lat : lat + 128] = jnp.where(lanes((own, 128)) < 64, new_key.astype(F32), 0.0)

    take_kv(rb2, 1)
    total = rb2[0].astype(F32)
    for j in range(1, n_kv):
        total = total + rb2[j].astype(F32)
    q_nope = total[:, 0:qw].astype(BF16)
    q_rope = rotate(total[:, qw : qw + 128], table)
    for h in range(2):
        spot = pl.ds(h, share, stride=2)
        put(f3, spot, dot(q_nope[:, 128 * h : 128 * (h + 1)], up_k[h], NT))
        turned = q_rope if h == 0 else pltpu.roll(q_rope, 64, 1)
        put(f3, spot, jnp.where(lanes((share, 128)) < 64, turned, 0.0), lat // 128)
    for i in range(share):
        sb3[i] = get(f3, slice(2 * i, 2 * i + 2)).astype(BF16)
    line, place = lax.rem(t, quarters), lax.div(t, quarters)
    stays = line == group

    @pl.loop(0, share)
    def _(i):
        to = quarters * i + group
        home = to == t

        @pl.when(jnp.logical_not(home))
        def _():
            send(sb3.at[i], rb3.at[place], tp_send.at[1], tp_recv.at[1], own * line + slot, to)

        @pl.when(home)
        def _():
            rb3[place] = sb3[i]

    by_head("vu", up_v)
    high, low = halves(jnp.sum(rows * rows, axis=1, keepdims=True))
    normed = (f1[...] * mlp_gain).astype(BF16)
    gate_up(normed)
    f10[:, padded - 128 : padded] = jnp.where(
        lane_row < 128 - free, f10[:, padded - 128 : padded], jnp.where(lane_row < 128 - free // 2, high, low)
    )
    for j in range(n_kv):
        sb_r[j] = f10[share * j : share * (j + 1), :].astype(BF16)
    over_kv(lambda to: sb_r.at[to], rb_r.at[k], 8)
    rb_r[k] = sb_r[k]

    @pl.when(stays)
    def _():
        take(rb3.at[pl.ds(0, tp_q - 1)], tp_recv.at[1])

    @pl.when(jnp.logical_not(stays))
    def _():
        take(rb3, tp_recv.at[1])

    for j in range(tp_q):
        fq[2 * j : 2 * j + 2, :] = rb3[j].astype(F32)
    part = pl.ds(pl.multiple_of(group * heads_q, heads_q), heads_q)
    rb_q[slot, part, :] = fq[...].astype(BF16)
    over_kv(lambda to: rb_q.at[slot, part], rb_q.at[slot, part], 2, q_recv.at[slot])

    loads["cl"].wait()
    loads["cr"].wait()
    for s in range(own):
        @pl.when(slot == s)
        def _():
            if quarters > 1:
                take(rb_q.at[s, pl.ds(0, heads_q * (quarters - 1))], q_recv.at[s])

        @pl.when(slot != s)
        def _():
            take(rb_q.at[s], q_recv.at[s])

        keys = v["cl"][s]
        scores = (dot(rb_q[s, :, 0:lat], keys, NT) + dot(rb_q[s, :, lat : lat + 64], v["cr"][s])) * factors[s : s + 1, 0:1]
        peak_high, peak_low = halves(jnp.max(scores, axis=1, keepdims=True))
        probs = jnp.exp(scores - (peak_high + peak_low))
        sum_high, sum_low = halves(jnp.sum(probs, axis=1, keepdims=True))
        sb4[s, :, 0:lat] = dot(probs.astype(BF16), keys).astype(BF16)
        lane = lanes((heads, 128))
        sb4[s, :, lat : lat + 128] = jnp.where(
            lane < 32, peak_high, jnp.where(lane < 64, peak_low, jnp.where(lane < 96, sum_high, sum_low))
        ).astype(BF16)
        for q in range(quarters):
            to = own * q + s

            @pl.when(k != to)
            def _():
                send(sb4.at[s, pl.ds(heads_q * q, heads_q)], rb4.at[k], kv_send.at[3], kv_recv.at[3], to, t)

            @pl.when(k == to)
            def _():
                rb4[k] = sb4[s, heads_q * q : heads_q * (q + 1), :]

    query = rb_q[slot, part, :].astype(F32)
    mine = nl[pl.ds(slot, 1), :]
    own_score = jnp.sum(query * mine, axis=1, keepdims=True) * factors[pl.ds(slot, 1), :][:, 0:1]
    take_kv(rb4, 3)
    peaks, sums = [], []
    top = own_score
    for j in range(n_kv):
        stats = rb4[j, :, lat : lat + 128].astype(F32)
        peaks.append(stats[:, 0:1] + stats[:, 32:33])
        sums.append(stats[:, 64:65] + stats[:, 96:97])
        top = jnp.maximum(top, peaks[-1])
    own_prob = jnp.exp(own_score - top)
    totals = own_prob
    summed = own_prob * mine[:, 0:lat]
    for j in range(n_kv):
        weight = jnp.exp(peaks[j] - top)
        totals = totals + sums[j] * weight
        summed = summed + rb4[j, :, 0:lat].astype(F32) * weight
    f5[...] = summed / totals
    for i in range(tp_q):
        sb5[i] = f5[2 * i : 2 * i + 2, :].astype(BF16)

    @pl.loop(0, tp_q)
    def _(i):
        to = quarters * i + group

        @pl.when(to != t)
        def _():
            send(sb5.at[i], rb5.at[t], tp_send.at[2], tp_recv.at[2], k, to)

        @pl.when(to == t)
        def _():
            rb5[t] = sb5[i]

    take_kv(rb_r, 8)
    total = rb_r[0].astype(F32)
    for j in range(1, n_kv):
        total = total + rb_r[j].astype(F32)
    sum_r[...] = total
    gathers_o = line == group

    @pl.when(gathers_o)
    def _():
        take_tp(rb5, 2)
        for j in range(n_tp):
            put(fo, slice(2 * j, 2 * j + 2), rb5[j].astype(F32))
        terms = [dot(get(fo, pl.ds(h, n_tp, stride=2)).astype(BF16), up_v[h]).astype(BF16) for h in range(2)]
        rb6[slot] = jnp.concatenate(terms, axis=1)
        over_kv(lambda to: rb6.at[slot], rb6.at[slot], 4, o_recv.at[slot])

    for s in range(own):
        @pl.when(k != own * line + s)
        def _():
            take(rb6.at[s], o_recv.at[s])

        put(f7, slice(n_tp * s, n_tp * (s + 1)), dot(rb6[s], v["wo"][...]))
    for j in range(n_tp):
        sb7[j] = get(f7, pl.ds(j, own, stride=n_tp)).astype(BF16)
    over_tp(lambda to: sb7.at[to], rb7.at[t], 3)
    rb7[t] = sb7[t]
    take_tp(rb7, 3)
    attended = jnp.sum(rb7[...].astype(F32), axis=0)
    sb8[...] = jnp.broadcast_to(jnp.sum(attended * attended, axis=1, keepdims=True), sb8.shape)
    over_kv(lambda to: sb8, rb8.at[k], 5)
    rb8[k] = sb8[...]
    mid[...] = attended.astype(BF16)
    over_tp(lambda to: mid, rb9.at[t], 4)
    rb9[t] = mid[...]
    take_tp(rb9, 4)
    for j in range(n_tp):
        f2r[own * j : own * (j + 1), :] = rb9[j].astype(F32)
    rows = f2r[...]
    post = rows * post_gain
    gate_up((post * mlp_gain).astype(BF16))
    stats = []
    for product in (rows * rows, f1[...] * post, post * post):
        stats.extend(halves(jnp.sum(product, axis=1, keepdims=True)))
    for at, picks in ((padded, stats[0:4]), (2 * padded, stats[4:6])):
        tile = f10[:, at - 128 : at]
        for n, pick in enumerate(picks):
            tile = jnp.where(lane_row >= 128 - free + n * (free // len(picks)), pick, tile)
        f10[:, at - 128 : at] = tile
    for j in range(n_kv):
        sb10[j] = f10[share * j : share * (j + 1), :].astype(BF16)
    over_kv(lambda to: sb10.at[to], rb10.at[k], 6)
    rb10[k] = sb10[k]
    take_kv(rb10, 6)
    total = rb10[0].astype(F32)
    for j in range(1, n_kv):
        total = total + rb10[j].astype(F32)
    base = sum_r[...]
    quarter = free // 4

    def stat(value, at, width):
        return value[:, at : at + 1] + value[:, at + width : at + width + 1]

    resid_square = stat(base, ff, free // 2)
    factor = lax.rsqrt(stat(total, ff, quarter) / model + EPS)
    mixed = stat(total, ff + 2 * quarter, quarter)
    post_sum = stat(total, padded + ff, free // 2)
    mid_square = jnp.maximum(resid_square + factor * (2.0 * mixed + factor * post_sum), 0.0)
    scale_mid = lax.rsqrt(mid_square / model + EPS)
    both = (base + factor * total) * scale_mid
    gate, up = both[:, 0:padded], both[:, padded : 2 * padded]
    hidden = gate / (1.0 + jnp.exp(-gate)) * up
    sb11[...] = jnp.where(lanes((share, padded)) < ff, hidden, 0.0).astype(BF16)
    over_kv(lambda to: sb11, rb11.at[k], 7)
    rb11[k] = sb11[...]
    take_kv(rb11, 7)
    everything = rb11[...].astype(F32).reshape(batch, padded).astype(BF16)
    f1[...] = dot(everything[:, 0:ff], v["wd"][...])
    for j in range(n_tp):
        sb12[j] = f1[own * j : own * (j + 1), :].astype(BF16)
    over_tp(lambda to: sb12.at[to], rb12.at[t], 5)
    rb12[t] = sb12[t]
    take_kv(rb8, 5)
    post_square = jnp.sum(rb8[...], axis=0)[:, 0:1]
    resid_mid = (resid + attended * lax.rsqrt(post_square / model + EPS) * post_gain).astype(BF16).astype(F32)
    take_tp(rb12, 5)
    out[:, 0:width] = resid_mid + jnp.sum(rb12[...].astype(F32), axis=0)

    for phase, ref in ((0, rb1), (3, rb7), (4, rb9), (5, rb12)):
        take(ref.at[pl.ds(0, n_tp - 1)], tp_send.at[phase])
    for phase, ref in ((0, rb_l), (1, rb2), (3, rb4), (5, rb8), (6, rb10), (7, rb11), (8, rb_r)):
        take(ref.at[pl.ds(0, n_kv - 1)], kv_send.at[phase])
    for phase, ref, count, inside in ((1, sb3, share, stays), (2, rb5, tp_q, gathers_o)):
        @pl.when(inside)
        def _():
            take(ref.at[pl.ds(0, count - 1)], tp_send.at[phase])

        @pl.when(jnp.logical_not(inside))
        def _():
            take(ref.at[pl.ds(0, count)], tp_send.at[phase])

    take(rb4.at[pl.ds(0, n_kv - 1)], kv_send.at[2])

    @pl.when(gathers_o)
    def _():
        @pl.loop(1, n_kv)
        def _(i):
            take(rb6.at[0], kv_send.at[4])


def split(parts, whole, *outs):
    for (start, size), out in zip(parts, outs):
        out[...] = whole[:, start : start + size].astype(BF16)


def body(
    resid, attn_gain, w_query_nope, w_query_rope, w_latent, w_key_rope, latent_gain, key_up, value_up,
    w_out, post_gain, mlp_gain, w_gate, w_up, w_down, cache_latent, cache_rope_key,
):
    n_kv, n_tp = lax.axis_size("kv"), lax.axis_size("tp")
    own, width = resid.shape
    batch, share = own * n_tp, own * n_tp // n_kv
    lat, positions = cache_latent.shape[2], cache_latent.shape[1]
    quarters = n_kv // own
    heads = 2 * n_tp
    heads_q, tp_q = heads // quarters, n_tp // quarters
    ff = w_gate.shape[1]
    padded = -(-ff // 128) * 128
    qw = w_query_nope.shape[1]
    operands = (
        resid,
        attn_gain.reshape(-1, 128),
        post_gain.reshape(-1, 128),
        mlp_gain.reshape(-1, 128),
        latent_gain.reshape(-1, 128),
        jnp.asarray(rotation_table(positions * n_kv)),
        w_query_nope,
        w_query_rope,
        w_latent,
        w_key_rope.T,
        key_up,
        value_up,
        w_out,
        w_gate.T,
        w_up.T,
        w_down,
        cache_latent,
        cache_rope_key.swapaxes(1, 2),
    )
    local = [pltpu.VMEM(o.shape, o.dtype) for o in operands]
    local[9] = pltpu.VMEM((64, width), BF16)
    wide = lat + 128
    dma = pltpu.SemaphoreType.DMA
    scratch = local + [
        dma((len(INPUTS),)),
        pltpu.VMEM((batch, width), F32),
        pltpu.VMEM((own, wide), F32),
        pltpu.VMEM((n_kv, own, wide), F32),
        pltpu.VMEM((n_tp, own, width), BF16),
        pltpu.VMEM((qw // 128 + 1, batch, 128), F32),
        pltpu.VMEM((n_kv, share, qw + 128), BF16),
        pltpu.VMEM((n_kv, share, qw + 128), BF16),
        pltpu.VMEM((wide // 128, 2 * share, 128), F32),
        pltpu.VMEM((share, 2, wide), BF16),
        pltpu.VMEM((tp_q, 2, wide), BF16),
        pltpu.VMEM((heads_q, wide), F32),
        pltpu.VMEM((own, heads, wide), BF16),
        pltpu.VMEM((own, heads, wide), BF16),
        pltpu.VMEM((n_kv, heads_q, wide), BF16),
        pltpu.VMEM((heads_q, lat), F32),
        pltpu.VMEM((tp_q, 2, lat), BF16),
        pltpu.VMEM((n_tp, 2, lat), BF16),
        pltpu.VMEM((lat // 128, heads, 128), F32),
        pltpu.VMEM((own, n_tp, 256), BF16),
        pltpu.VMEM((width // 128, batch, 128), F32),
        pltpu.VMEM((n_tp, own, width), BF16),
        pltpu.VMEM((n_tp, own, width), BF16),
        pltpu.VMEM((own, 128), F32),
        pltpu.VMEM((n_kv, own, 128), F32),
        pltpu.VMEM((own, width), BF16),
        pltpu.VMEM((n_tp, own, width), BF16),
        pltpu.VMEM((batch, 2 * padded), F32),
        pltpu.VMEM((n_kv, share, 2 * padded), BF16),
        pltpu.VMEM((n_kv, share, 2 * padded), BF16),
        pltpu.VMEM((n_kv, share, 2 * padded), BF16),
        pltpu.VMEM((n_kv, share, 2 * padded), BF16),
        pltpu.VMEM((share, 2 * padded), F32),
        pltpu.VMEM((batch, width), F32),
        pltpu.VMEM((share, padded), BF16),
        pltpu.VMEM((n_kv, share, padded), BF16),
        pltpu.VMEM((n_tp, own, width), BF16),
        pltpu.VMEM((n_tp, own, width), BF16),
        pltpu.VMEM((attn_gain.shape[0] // 128, 128), F32),
        pltpu.VMEM((own, wide), F32),
        pltpu.VMEM((2 * lat, 128), F32),
        pltpu.VMEM((2, lat, 128), BF16),
        pltpu.VMEM((2, lat, 128), BF16),
        pltpu.VMEM((own, 128), F32),
        dma((6,)),
        dma((6,)),
        dma((9,)),
        dma((9,)),
        dma((own,)),
        dma((own,)),
    ]
    out = pl.pallas_call(
        functools.partial(kernel, n_kv, n_tp),
        out_shape=jax.ShapeDtypeStruct((own, width + wide), F32),
        in_specs=[pl.BlockSpec(memory_space=pl.ANY)] * len(operands),
        out_specs=pl.BlockSpec(memory_space=pltpu.VMEM),
        scratch_shapes=scratch,
        compiler_params=pltpu.CompilerParams(
            collective_id=0, has_side_effects=True, vmem_limit_bytes=67043328
        ),
    )(*operands)
    parts = ((0, width), (width, lat), (width + lat, 64))
    return pl.pallas_call(
        functools.partial(split, parts),
        out_shape=tuple(jax.ShapeDtypeStruct((own, size), BF16) for _, size in parts),
        in_specs=[pl.BlockSpec(memory_space=pltpu.VMEM)],
        out_specs=(pl.BlockSpec(memory_space=pltpu.VMEM),) * 3,
    )(out)


def solution(mesh):
    placed = (
        P("tp", "kv"),
        P(),
        P("kv", "tp"),
        P("kv", "tp"),
        P("kv", None),
        P(),
        P(),
        P(None, "tp", None),
        P(None, "tp", None),
        P("tp", "kv"),
        P(),
        P(),
        P("kv", "tp"),
        P("kv", "tp"),
        P("tp", "kv"),
        P("tp", "kv", None),
        P("tp", "kv", None),
    )
    return jax.shard_map(
        body,
        mesh=mesh,
        in_specs=placed,
        out_specs=(P("tp", "kv"), P("tp", None), P("tp", None)),
        check_vma=False,
    )
```

```python
import functools

import jax
import jax.numpy as jnp
import numpy as np
from jax import lax
from jax.experimental import pallas as pl
from jax.experimental.pallas import tpu as pltpu
from jax.sharding import PartitionSpec as P

EPS = 1e-06
THETA = 10000.0
MESH = pl.DeviceIdType.MESH
F32 = jnp.float32
BF16 = jnp.bfloat16
NN = (((1,), (0,)), ((), ()))
NT = (((1,), (1,)), ((), ()))


def dot(a, b, dims=NN):
    return lax.dot_general(a, b, dims, preferred_element_type=F32)


def halves(value):
    high = value.astype(BF16).astype(F32)
    return high, (value - high).astype(BF16).astype(F32)


def put(ref, rows, value, first=0):
    for c in range(value.shape[1] // 128):
        ref[first + c, rows, :] = value[:, 128 * c : 128 * (c + 1)]


def get(ref, rows):
    return jnp.concatenate([ref[c, rows, :] for c in range(ref.shape[0])], axis=1)


def lanes(shape):
    return lax.broadcasted_iota(jnp.int32, shape, len(shape) - 1)


def rotate(vector, table):
    lower = lanes(vector.shape) % 64 < 32
    partner = jnp.where(lower, pltpu.roll(vector, 96, 1), pltpu.roll(vector, 32, 1))
    return vector * table[0:1, :] + partner * table[1:2, :]


def rotation_table(position):
    frequency = THETA ** (-np.arange(32, dtype=np.float64) / 32)
    angles = position * frequency
    cos, sin = np.cos(angles), np.sin(angles)
    return np.stack(
        [np.tile(np.concatenate([cos, cos]), 2), np.tile(np.concatenate([-sin, sin]), 2)]
    ).astype(np.float32)


INPUTS = (
    "resid",
    "attn_gain",
    "post_gain",
    "mlp_gain",
    "latent_gain",
    "table",
    "wqn",
    "wqr",
    "wl",
    "wkr",
    "ku",
    "vu",
    "wo",
    "wg",
    "wu",
    "wd",
    "cl",
    "cr",
)


def kernel(n_kv, n_tp, *refs):
    n_in = len(INPUTS)
    hbm = dict(zip(INPUTS, refs[:n_in]))
    out = refs[n_in]
    scratch = refs[n_in + 1 :]
    v = dict(zip(INPUTS, scratch[:n_in]))
    (
        load_sem,
        f1, sb_l, rb_l, rb1, f2, sb2, rb2, f3, sb3, rb3, fq, rb_q, sb4, rb4, f5, sb5, rb5, fo, rb6,
        f7, sb7, rb7, sb8, rb8, mid, rb9, f10, sb10, rb10, sb_r, rb_r, sum_r, f2r, sb11, rb11, rb12, sb12, g1, nl, pairs, up_k, up_v, factors,
        tp_send, tp_recv, kv_send, kv_recv, q_recv, o_recv,
    ) = scratch[n_in:]

    k, t = lax.axis_index("kv"), lax.axis_index("tp")
    own = v["resid"].shape[0]
    batch = own * n_tp
    width = v["resid"].shape[1]
    model = width * n_kv
    lat = v["cl"].shape[2]
    quarters = n_kv // own
    share = batch // n_kv
    heads = 2 * n_tp
    heads_q = heads // quarters
    tp_q = n_tp // quarters
    ff = v["wg"].shape[0]
    scale = (128 + 64) ** (-0.5)
    padded = -(-ff // 128) * 128
    free = padded - ff
    lane_row = lanes((batch, 128))
    slot, group = lax.rem(k, own), lax.div(k, own)

    around = [n_tp // 2 + (i + 1) // 2 * (1 - 2 * (i % 2)) for i in range(n_tp - 1)]
    far_tp = [lax.rem(t + offset, n_tp) for offset in around]
    rows_kv = n_kv // own
    steps = [(y, x) for y in range(rows_kv) for x in range(own) if (y, x) != (0, 0)]
    steps.sort(key=lambda step: -min(step[0], rows_kv - step[0]) - min(step[1], own - step[1]))
    far_kv = [lax.rem(group + y, rows_kv) * own + lax.rem(slot + x, own) for y, x in steps]

    first = pltpu.make_async_copy(hbm["resid"], v["resid"], load_sem.at[0])
    first.start()
    barrier = pltpu.get_barrier_semaphore()

    for to in far_tp:
        pl.semaphore_signal(barrier, inc=1, device_id={"kv": k, "tp": to}, device_id_type=MESH)
    for to in far_kv:
        pl.semaphore_signal(barrier, inc=1, device_id={"kv": to, "tp": t}, device_id_type=MESH)

    loads = {}
    for at, name in enumerate(INPUTS):
        source = hbm[name]
        if name == "wkr":
            source = source.at[:, pl.ds(pl.multiple_of(k * width, width), width)]
        loads[name] = first if name == "resid" else pltpu.make_async_copy(source, v[name], load_sem.at[at])
        if name != "resid":
            loads[name].start()

    def send(src, dst, send_sem, recv_sem, kv, tp):
        pltpu.make_async_remote_copy(
            src_ref=src,
            dst_ref=dst,
            send_sem=send_sem,
            recv_sem=recv_sem,
            device_id={"kv": kv, "tp": tp},
            device_id_type=MESH,
        ).start()

    def over_tp(src_of, dst, phase):
        for to in far_tp:
            send(src_of(to), dst, tp_send.at[phase], tp_recv.at[phase], k, to)

    def over_kv(src_of, dst, phase, recv=None):
        for to in far_kv:
            send(src_of(to), dst, kv_send.at[phase], kv_recv.at[phase] if recv is None else recv, to, t)

    def by_head(name, to):
        @pl.loop(0, lat, unroll=16)
        def _(c):
            pairs[pl.ds(2 * c, 2), :] = v[name][c].astype(F32)

        for h in range(2):
            to[h] = pairs[pl.ds(h, lat, stride=2), :].astype(BF16)

    def gate_up(rows):
        f10[:, 2 * padded - 128 : 2 * padded] = jnp.zeros((batch, 128), F32)
        f10[:, 0:ff] = dot(rows, v["wg"][...], NT)
        f10[:, padded : padded + ff] = dot(rows, v["wu"][...], NT)

    def take(ref, sem):
        pltpu.make_async_copy(ref, ref, sem).wait()

    def take_tp(ref, phase):
        take(ref.at[pl.ds(0, n_tp - 1)], tp_recv.at[phase])

    def take_kv(ref, phase):
        take(ref.at[pl.ds(0, n_kv - 1)], kv_recv.at[phase])

    first.wait()
    pl.semaphore_wait(barrier, n_tp + n_kv - 2)

    over_tp(lambda to: v["resid"], rb1.at[t], 0)
    rb1[t] = v["resid"][...]
    for name in ("attn_gain", "post_gain", "mlp_gain", "wl", "wkr", "latent_gain", "table"):
        loads[name].wait()

    def block_of(name):
        g1[...] = v[name][...].astype(F32)
        per = width // 128
        return jnp.concatenate([g1[pl.ds(k * per + j, 1), :] for j in range(per)], axis=1)

    attn_gain, post_gain, mlp_gain = block_of("attn_gain"), block_of("post_gain"), block_of("mlp_gain")
    resid = v["resid"][...].astype(F32)
    own_normed = (resid * attn_gain).astype(BF16)
    sb_l[:, 0:lat] = dot(own_normed, v["wl"][...])
    key_part = dot(own_normed, v["wkr"][...], NT)
    square = jnp.sum(resid * resid, axis=1, keepdims=True)
    sb_l[:, lat : lat + 128] = jnp.concatenate([key_part, jnp.broadcast_to(square, (own, 64))], axis=1)
    over_kv(lambda to: sb_l, rb_l.at[k], 0)
    rb_l[k] = sb_l[...]
    for name in INPUTS:
        if name in ("wqn", "wqr", "ku", "vu", "wo", "wg", "wu", "wd"):
            loads[name].wait()
    by_head("ku", up_k)
    take_tp(rb1, 0)
    for j in range(n_tp):
        f1[own * j : own * (j + 1), :] = rb1[j].astype(F32)
    rows = f1[...]
    normed = (rows * attn_gain).astype(BF16)
    qw = v["wqn"].shape[1]
    every = slice(None)
    put(f2, every, dot(normed, v["wqn"][...]))
    put(f2, every, dot(normed, v["wqr"][...]), qw // 128)
    for j in range(n_kv):
        sb2[j] = get(f2, pl.ds(j, share, stride=n_kv)).astype(BF16)
    over_kv(lambda to: sb2.at[to], rb2.at[k], 1)
    rb2[k] = sb2[k]

    take_kv(rb_l, 0)
    total = rb_l[0]
    for j in range(1, n_kv):
        total = total + rb_l[j]
    latent = total[:, 0:lat]
    gain_rows = v["latent_gain"][...].astype(F32)
    latent_gain = jnp.concatenate([gain_rows[j : j + 1, :] for j in range(lat // 128)], axis=1)
    new_latent = (
        latent * lax.rsqrt(jnp.mean(latent * latent, axis=1, keepdims=True) + EPS) * latent_gain
    ).astype(BF16)
    out[:, width : width + lat] = new_latent.astype(F32)
    key = total[:, lat : lat + 128]
    own_scale = lax.rsqrt(key[:, 64:65] / model + EPS)
    table = v["table"][...]
    new_key = rotate(key * own_scale, table).astype(BF16)
    out[:, width + lat : width + lat + 128] = new_key.astype(F32)
    factors[...] = jnp.broadcast_to(own_scale * scale, factors.shape)
    nl[:, 0:lat] = new_latent.astype(F32)
    nl[:, lat : lat + 128] = jnp.where(lanes((own, 128)) < 64, new_key.astype(F32), 0.0)

    take_kv(rb2, 1)
    total = rb2[0].astype(F32)
    for j in range(1, n_kv):
        total = total + rb2[j].astype(F32)
    q_nope = total[:, 0:qw].astype(BF16)
    q_rope = rotate(total[:, qw : qw + 128], table)
    for h in range(2):
        spot = pl.ds(h, share, stride=2)
        put(f3, spot, dot(q_nope[:, 128 * h : 128 * (h + 1)], up_k[h], NT))
        turned = q_rope if h == 0 else pltpu.roll(q_rope, 64, 1)
        put(f3, spot, jnp.where(lanes((share, 128)) < 64, turned, 0.0), lat // 128)
    for i in range(share):
        sb3[i] = get(f3, slice(2 * i, 2 * i + 2)).astype(BF16)
    line, place = lax.rem(t, quarters), lax.div(t, quarters)
    stays = line == group

    @pl.loop(0, share)
    def _(i):
        to = quarters * i + group
        home = to == t

        @pl.when(jnp.logical_not(home))
        def _():
            send(sb3.at[i], rb3.at[place], tp_send.at[1], tp_recv.at[1], own * line + slot, to)

        @pl.when(home)
        def _():
            rb3[place] = sb3[i]

    by_head("vu", up_v)
    @pl.when(stays)
    def _():
        take(rb3.at[pl.ds(0, tp_q - 1)], tp_recv.at[1])

    @pl.when(jnp.logical_not(stays))
    def _():
        take(rb3, tp_recv.at[1])

    for j in range(tp_q):
        fq[2 * j : 2 * j + 2, :] = rb3[j].astype(F32)
    part = pl.ds(pl.multiple_of(group * heads_q, heads_q), heads_q)
    rb_q[slot, part, :] = fq[...].astype(BF16)
    over_kv(lambda to: rb_q.at[slot, part], rb_q.at[slot, part], 2, q_recv.at[slot])

    loads["cl"].wait()
    loads["cr"].wait()
    def scores_of(s):
        @pl.when(slot == s)
        def _():
            if quarters > 1:
                take(rb_q.at[s, pl.ds(0, heads_q * (quarters - 1))], q_recv.at[s])

        @pl.when(slot != s)
        def _():
            take(rb_q.at[s], q_recv.at[s])

        found = dot(rb_q[s, :, 0:lat], v["cl"][s], NT) + dot(rb_q[s, :, lat : lat + 64], v["cr"][s])
        return found * factors[s : s + 1, 0:1]

    following = scores_of(0)
    for s in range(own):
        scores = following
        if s + 1 < own:
            following = scores_of(s + 1)
        peak_high, peak_low = halves(jnp.max(scores, axis=1, keepdims=True))
        probs = jnp.exp(scores - (peak_high + peak_low))
        sum_high, sum_low = halves(jnp.sum(probs, axis=1, keepdims=True))
        sb4[s, :, 0:lat] = dot(probs.astype(BF16), v["cl"][s]).astype(BF16)
        lane = lanes((heads, 128))
        sb4[s, :, lat : lat + 128] = jnp.where(
            lane < 32, peak_high, jnp.where(lane < 64, peak_low, jnp.where(lane < 96, sum_high, sum_low))
        ).astype(BF16)
        for q in range(quarters):
            to = own * q + s

            @pl.when(k != to)
            def _():
                send(sb4.at[s, pl.ds(heads_q * q, heads_q)], rb4.at[k], kv_send.at[3], kv_recv.at[3], to, t)

            @pl.when(k == to)
            def _():
                rb4[k] = sb4[s, heads_q * q : heads_q * (q + 1), :]

    query = rb_q[slot, part, :].astype(F32)
    mine = nl[pl.ds(slot, 1), :]
    own_score = jnp.sum(query * mine, axis=1, keepdims=True) * factors[pl.ds(slot, 1), :][:, 0:1]
    take_kv(rb4, 3)
    peaks, sums = [], []
    top = own_score
    for j in range(n_kv):
        stats = rb4[j, :, lat : lat + 128].astype(F32)
        peaks.append(stats[:, 0:1] + stats[:, 32:33])
        sums.append(stats[:, 64:65] + stats[:, 96:97])
        top = jnp.maximum(top, peaks[-1])
    own_prob = jnp.exp(own_score - top)
    totals = own_prob
    summed = own_prob * mine[:, 0:lat]
    for j in range(n_kv):
        weight = jnp.exp(peaks[j] - top)
        totals = totals + sums[j] * weight
        summed = summed + rb4[j, :, 0:lat].astype(F32) * weight
    f5[...] = summed / totals
    for i in range(tp_q):
        sb5[i] = f5[2 * i : 2 * i + 2, :].astype(BF16)

    @pl.loop(0, tp_q)
    def _(i):
        to = quarters * i + group

        @pl.when(to != t)
        def _():
            send(sb5.at[i], rb5.at[t], tp_send.at[2], tp_recv.at[2], k, to)

        @pl.when(to == t)
        def _():
            rb5[t] = sb5[i]

    rows = f1[...]
    high, low = halves(jnp.sum(rows * rows, axis=1, keepdims=True))
    normed = (rows * mlp_gain).astype(BF16)
    gate_up(normed)
    f10[:, padded - 128 : padded] = jnp.where(
        lane_row < 128 - free, f10[:, padded - 128 : padded], jnp.where(lane_row < 128 - free // 2, high, low)
    )
    for j in range(n_kv):
        sb_r[j] = f10[share * j : share * (j + 1), :].astype(BF16)
    over_kv(lambda to: sb_r.at[to], rb_r.at[k], 8)
    rb_r[k] = sb_r[k]

    gathers_o = line == group

    @pl.when(gathers_o)
    def _():
        take_tp(rb5, 2)
        for j in range(n_tp):
            put(fo, slice(2 * j, 2 * j + 2), rb5[j].astype(F32))
        terms = [dot(get(fo, pl.ds(h, n_tp, stride=2)).astype(BF16), up_v[h]).astype(BF16) for h in range(2)]
        rb6[slot] = jnp.concatenate(terms, axis=1)
        over_kv(lambda to: rb6.at[slot], rb6.at[slot], 4, o_recv.at[slot])

    for s in range(own):
        @pl.when(k != own * line + s)
        def _():
            take(rb6.at[s], o_recv.at[s])

        put(f7, slice(n_tp * s, n_tp * (s + 1)), dot(rb6[s], v["wo"][...]))
    for j in range(n_tp):
        sb7[j] = get(f7, pl.ds(j, own, stride=n_tp)).astype(BF16)
    over_tp(lambda to: sb7.at[to], rb7.at[t], 3)
    rb7[t] = sb7[t]
    take_kv(rb_r, 8)
    total = rb_r[0].astype(F32)
    for j in range(1, n_kv):
        total = total + rb_r[j].astype(F32)
    sum_r[...] = total
    take_tp(rb7, 3)
    attended = jnp.sum(rb7[...].astype(F32), axis=0)
    mid[...] = attended.astype(BF16)
    over_tp(lambda to: mid, rb9.at[t], 4)
    rb9[t] = mid[...]
    sb8[...] = jnp.broadcast_to(jnp.sum(attended * attended, axis=1, keepdims=True), sb8.shape)
    over_kv(lambda to: sb8, rb8.at[k], 5)
    rb8[k] = sb8[...]
    take_tp(rb9, 4)
    for j in range(n_tp):
        f2r[own * j : own * (j + 1), :] = rb9[j].astype(F32)
    rows = f2r[...]
    post = rows * post_gain
    gate_up((post * mlp_gain).astype(BF16))
    stats = []
    for product in (rows * rows, f1[...] * post, post * post):
        stats.extend(halves(jnp.sum(product, axis=1, keepdims=True)))
    for at, picks in ((padded, stats[0:4]), (2 * padded, stats[4:6])):
        tile = f10[:, at - 128 : at]
        for n, pick in enumerate(picks):
            tile = jnp.where(lane_row >= 128 - free + n * (free // len(picks)), pick, tile)
        f10[:, at - 128 : at] = tile
    for j in range(n_kv):
        sb10[j] = f10[share * j : share * (j + 1), :].astype(BF16)
    over_kv(lambda to: sb10.at[to], rb10.at[k], 6)
    rb10[k] = sb10[k]
    take_kv(rb10, 6)
    total = rb10[0].astype(F32)
    for j in range(1, n_kv):
        total = total + rb10[j].astype(F32)
    base = sum_r[...]
    quarter = free // 4

    def stat(value, at, width):
        return value[:, at : at + 1] + value[:, at + width : at + width + 1]

    resid_square = stat(base, ff, free // 2)
    factor = lax.rsqrt(stat(total, ff, quarter) / model + EPS)
    mixed = stat(total, ff + 2 * quarter, quarter)
    post_sum = stat(total, padded + ff, free // 2)
    mid_square = jnp.maximum(resid_square + factor * (2.0 * mixed + factor * post_sum), 0.0)
    scale_mid = lax.rsqrt(mid_square / model + EPS)
    both = (base + factor * total) * scale_mid
    gate, up = both[:, 0:padded], both[:, padded : 2 * padded]
    hidden = gate / (1.0 + jnp.exp(-gate)) * up
    sb11[...] = jnp.where(lanes((share, padded)) < ff, hidden, 0.0).astype(BF16)
    over_kv(lambda to: sb11, rb11.at[k], 7)
    rb11[k] = sb11[...]
    take_kv(rb11, 7)
    everything = rb11[...].astype(F32).reshape(batch, padded).astype(BF16)
    f1[...] = dot(everything[:, 0:ff], v["wd"][...])
    for j in range(n_tp):
        sb12[j] = f1[own * j : own * (j + 1), :].astype(BF16)
    over_tp(lambda to: sb12.at[to], rb12.at[t], 5)
    rb12[t] = sb12[t]
    take_kv(rb8, 5)
    post_square = jnp.sum(rb8[...], axis=0)[:, 0:1]
    resid_mid = (resid + attended * lax.rsqrt(post_square / model + EPS) * post_gain).astype(BF16).astype(F32)
    take_tp(rb12, 5)
    out[:, 0:width] = resid_mid + jnp.sum(rb12[...].astype(F32), axis=0)

    for phase, ref in ((0, rb1), (3, rb7), (4, rb9), (5, rb12)):
        take(ref.at[pl.ds(0, n_tp - 1)], tp_send.at[phase])
    for phase, ref in ((0, rb_l), (1, rb2), (3, rb4), (5, rb8), (6, rb10), (7, rb11), (8, rb_r)):
        take(ref.at[pl.ds(0, n_kv - 1)], kv_send.at[phase])
    for phase, ref, count, inside in ((1, sb3, share, stays), (2, rb5, tp_q, gathers_o)):
        @pl.when(inside)
        def _():
            take(ref.at[pl.ds(0, count - 1)], tp_send.at[phase])

        @pl.when(jnp.logical_not(inside))
        def _():
            take(ref.at[pl.ds(0, count)], tp_send.at[phase])

    take(rb4.at[pl.ds(0, n_kv - 1)], kv_send.at[2])

    @pl.when(gathers_o)
    def _():
        @pl.loop(1, n_kv)
        def _(i):
            take(rb6.at[0], kv_send.at[4])


def split(parts, whole, *outs):
    for (start, size), out in zip(parts, outs):
        out[...] = whole[:, start : start + size].astype(BF16)


def body(
    resid, attn_gain, w_query_nope, w_query_rope, w_latent, w_key_rope, latent_gain, key_up, value_up,
    w_out, post_gain, mlp_gain, w_gate, w_up, w_down, cache_latent, cache_rope_key,
):
    n_kv, n_tp = lax.axis_size("kv"), lax.axis_size("tp")
    own, width = resid.shape
    batch, share = own * n_tp, own * n_tp // n_kv
    lat, positions = cache_latent.shape[2], cache_latent.shape[1]
    quarters = n_kv // own
    heads = 2 * n_tp
    heads_q, tp_q = heads // quarters, n_tp // quarters
    ff = w_gate.shape[1]
    padded = -(-ff // 128) * 128
    qw = w_query_nope.shape[1]
    operands = (
        resid,
        attn_gain.reshape(-1, 128),
        post_gain.reshape(-1, 128),
        mlp_gain.reshape(-1, 128),
        latent_gain.reshape(-1, 128),
        jnp.asarray(rotation_table(positions * n_kv)),
        w_query_nope,
        w_query_rope,
        w_latent,
        w_key_rope.T,
        key_up,
        value_up,
        w_out,
        w_gate.T,
        w_up.T,
        w_down,
        cache_latent,
        cache_rope_key.swapaxes(1, 2),
    )
    local = [pltpu.VMEM(o.shape, o.dtype) for o in operands]
    local[9] = pltpu.VMEM((64, width), BF16)
    wide = lat + 128
    dma = pltpu.SemaphoreType.DMA
    scratch = local + [
        dma((len(INPUTS),)),
        pltpu.VMEM((batch, width), F32),
        pltpu.VMEM((own, wide), F32),
        pltpu.VMEM((n_kv, own, wide), F32),
        pltpu.VMEM((n_tp, own, width), BF16),
        pltpu.VMEM((qw // 128 + 1, batch, 128), F32),
        pltpu.VMEM((n_kv, share, qw + 128), BF16),
        pltpu.VMEM((n_kv, share, qw + 128), BF16),
        pltpu.VMEM((wide // 128, 2 * share, 128), F32),
        pltpu.VMEM((share, 2, wide), BF16),
        pltpu.VMEM((tp_q, 2, wide), BF16),
        pltpu.VMEM((heads_q, wide), F32),
        pltpu.VMEM((own, heads, wide), BF16),
        pltpu.VMEM((own, heads, wide), BF16),
        pltpu.VMEM((n_kv, heads_q, wide), BF16),
        pltpu.VMEM((heads_q, lat), F32),
        pltpu.VMEM((tp_q, 2, lat), BF16),
        pltpu.VMEM((n_tp, 2, lat), BF16),
        pltpu.VMEM((lat // 128, heads, 128), F32),
        pltpu.VMEM((own, n_tp, 256), BF16),
        pltpu.VMEM((width // 128, batch, 128), F32),
        pltpu.VMEM((n_tp, own, width), BF16),
        pltpu.VMEM((n_tp, own, width), BF16),
        pltpu.VMEM((own, 128), F32),
        pltpu.VMEM((n_kv, own, 128), F32),
        pltpu.VMEM((own, width), BF16),
        pltpu.VMEM((n_tp, own, width), BF16),
        pltpu.VMEM((batch, 2 * padded), F32),
        pltpu.VMEM((n_kv, share, 2 * padded), BF16),
        pltpu.VMEM((n_kv, share, 2 * padded), BF16),
        pltpu.VMEM((n_kv, share, 2 * padded), BF16),
        pltpu.VMEM((n_kv, share, 2 * padded), BF16),
        pltpu.VMEM((share, 2 * padded), F32),
        pltpu.VMEM((batch, width), F32),
        pltpu.VMEM((share, padded), BF16),
        pltpu.VMEM((n_kv, share, padded), BF16),
        pltpu.VMEM((n_tp, own, width), BF16),
        pltpu.VMEM((n_tp, own, width), BF16),
        pltpu.VMEM((attn_gain.shape[0] // 128, 128), F32),
        pltpu.VMEM((own, wide), F32),
        pltpu.VMEM((2 * lat, 128), F32),
        pltpu.VMEM((2, lat, 128), BF16),
        pltpu.VMEM((2, lat, 128), BF16),
        pltpu.VMEM((own, 128), F32),
        dma((6,)),
        dma((6,)),
        dma((9,)),
        dma((9,)),
        dma((own,)),
        dma((own,)),
    ]
    out = pl.pallas_call(
        functools.partial(kernel, n_kv, n_tp),
        out_shape=jax.ShapeDtypeStruct((own, width + wide), F32),
        in_specs=[pl.BlockSpec(memory_space=pl.ANY)] * len(operands),
        out_specs=pl.BlockSpec(memory_space=pltpu.VMEM),
        scratch_shapes=scratch,
        compiler_params=pltpu.CompilerParams(
            collective_id=0, has_side_effects=True, vmem_limit_bytes=67043328
        ),
    )(*operands)
    parts = ((0, width), (width, lat), (width + lat, 64))
    return pl.pallas_call(
        functools.partial(split, parts),
        out_shape=tuple(jax.ShapeDtypeStruct((own, size), BF16) for _, size in parts),
        in_specs=[pl.BlockSpec(memory_space=pltpu.VMEM)],
        out_specs=(pl.BlockSpec(memory_space=pltpu.VMEM),) * 3,
    )(out)


def solution(mesh):
    placed = (
        P("tp", "kv"),
        P(),
        P("kv", "tp"),
        P("kv", "tp"),
        P("kv", None),
        P(),
        P(),
        P(None, "tp", None),
        P(None, "tp", None),
        P("tp", "kv"),
        P(),
        P(),
        P("kv", "tp"),
        P("kv", "tp"),
        P("tp", "kv"),
        P("tp", "kv", None),
        P("tp", "kv", None),
    )
    return jax.shard_map(
        body,
        mesh=mesh,
        in_specs=placed,
        out_specs=(P("tp", "kv"), P("tp", None), P("tp", None)),
        check_vma=False,
    )
```
